32 devices in a mesh: sp: 4 (over z), fs: 4 (over y, x), tp: 2 (over core).
Axes of the slice: x: 2, y: 2, z: 4, core: 2. Of those that a mesh axis runs over, the one named last changes fastest.
Arguments:
- tokens: bfloat16 [512, 2048], P(('sp', 'fs', 'tp')), may hold values from -16 to 16
- in_gain: float32 [2048], replicated, may hold values from 0.1 to 1.9
- ret_query: bfloat16 [2048, 1024], P(None, ('fs', 'tp')), may hold values from -0.125 to 0.125
- ret_key: bfloat16 [2048, 1024], P(None, ('fs', 'tp')), may hold values from -0.125 to 0.125
- ret_value: bfloat16 [2048, 1024], P(None, ('fs', 'tp')), may hold values from -0.125 to 0.125
- decay_log: float32 [8, 512], P(('fs', 'tp'), 'sp'), may hold values from -1 to 0
- init_state: bfloat16 [8, 128, 128], P(('fs', 'tp')), may hold values from -24 to 24
- ret_gain: float32 [1024], P(('fs', 'tp')), may hold values from 0.1 to 1.9
- diff_query: bfloat16 [2, 2048, 512], P(None, None, ('fs', 'tp')), may hold values from -1 to 1
- diff_key: bfloat16 [2, 2048, 512], P(None, None, ('fs', 'tp')), may hold values from -1 to 1
- diff_value: bfloat16 [2048, 1024], P(None, ('fs', 'tp')), may hold values from -0.125 to 0.125
- diff_lambda: float32 [8], P(('fs', 'tp')), may hold values from 0.3 to 0.8
- diff_gain: float32 [1024], P(('fs', 'tp')), may hold values from 0.1 to 1.9
- out_weight: bfloat16 [2, 1024, 2048], P(None, ('fs', 'tp'), 'sp'), may hold values from -0.125 to 0.125
Outputs:
- mixed: bfloat16 [512, 2048], P(('sp', 'fs', 'tp'))
The draws below stay inside these ranges and needn't reach their ends.
All inputs are finite; a program needn't handle non-finite values.
Results may differ from the reference program's by a relative error of at most 0.017.
Values may be sent and summed in bfloat16 or wider, within the bound.
No kernel may reach another device: no remote copies, remote signals or barrier semaphores. Data moves between devices by JAX's collectives and lax.ppermute only.
A program may use at most 64 MiB of HBM per device.

```python
import jax
import jax.numpy as jnp
from jax import lax

D = 2048
KEEPING_MIXERS = 8
DIFF_HEADS = 8
HEAD = 128
MAP = 64
RBLOCK = 128
SHARD_POSITIONS = 128
TOKEN_COUNT = 512
N_SP = 4


def draw_tokens(key, part):
    sample = jax.random.normal(jax.random.fold_in(key, 11), (TOKEN_COUNT, D), jnp.float32)
    return jnp.clip(sample, -16.0, 16.0).astype(jnp.bfloat16)


def projection_draw(key, salt):
    sample = jax.random.normal(jax.random.fold_in(key, salt), (2, D, DIFF_HEADS * MAP), jnp.float32) * (1.3 * D ** (-0.5))
    return jnp.clip(sample, -1.0, 1.0)


def draw_diff_query(key, part):
    return projection_draw(key, 21).astype(jnp.bfloat16)


def draw_diff_key(key, part):
    return projection_draw(key, 22).astype(jnp.bfloat16)


def draw_decay_log(key, part):
    head_shape = (KEEPING_MIXERS, 1)
    slow_share = 0.5
    slow_heads = jax.random.uniform(jax.random.fold_in(key, 31), head_shape) < slow_share
    fast_rate = jax.random.uniform(jax.random.fold_in(key, 32), head_shape, minval=1.0 / 60.0, maxval=1.0 / 30.0)
    slow_rate = jax.random.uniform(jax.random.fold_in(key, 33), head_shape, minval=0.05, maxval=0.3) / TOKEN_COUNT
    single_tick_fading = jnp.where(slow_heads, slow_rate, fast_rate)
    fading_multiplier = jax.random.uniform(jax.random.fold_in(key, 34), (1, TOKEN_COUNT // SHARD_POSITIONS, 1), minval=1.0, maxval=3.0)
    fading_multiplier = jnp.broadcast_to(fading_multiplier, (1, TOKEN_COUNT // SHARD_POSITIONS, SHARD_POSITIONS)).reshape(1, TOKEN_COUNT)
    spurt_clusters = jax.random.uniform(jax.random.fold_in(key, 35), (KEEPING_MIXERS, TOKEN_COUNT)) < 3.0 / TOKEN_COUNT
    fading_drops = jnp.log(jax.random.uniform(jax.random.fold_in(key, 36), (KEEPING_MIXERS, TOKEN_COUNT), minval=0.5, maxval=0.8))
    return -single_tick_fading * fading_multiplier + jnp.where(spurt_clusters, fading_drops, 0.0)


def level_of(key, extent, shards, smallest, largest):
    def one(axis_at, blocks):
        heights = jax.random.uniform(jax.random.fold_in(jax.random.fold_in(key, 6), axis_at), (blocks,), jnp.float32, smallest / len(shards), largest / len(shards))
        return jnp.repeat(jnp.exp(heights), extent[axis_at] // blocks).reshape((-1,) + (1,) * (len(extent) - axis_at - 1))

    level = one(*shards[0])
    for cut in shards[1:]:
        level = level * one(*cut)
    return level


def normal_values(rng, dims, spread, most, shards=(), kind=jnp.bfloat16):
    values = jax.random.normal(rng, dims, jnp.float32) * spread
    if len(shards) > 0:
        values = level_of(rng, dims, shards, -0.22, 0.18) * values
    return jnp.clip(values, min=-most, max=most).astype(kind)


def setup_inputs(seed: int = 0) -> dict:
    keys = jax.random.split(jax.random.key(seed), 15)
    return {
        "tokens": draw_tokens(jax.random.fold_in(keys[14], 71), 0),
        "in_gain": jnp.clip(1.0 + 0.18 * jax.random.normal(keys[1], (D,), jnp.float32), 0.1, 1.9),
        "ret_query": normal_values(keys[2], (D, KEEPING_MIXERS * HEAD), D ** -0.5, 0.125, ((1, 8),)),
        "ret_key": normal_values(keys[3], (D, KEEPING_MIXERS * HEAD), D ** -0.5, 0.125, ((1, 8),)),
        "ret_value": normal_values(keys[4], (D, KEEPING_MIXERS * HEAD), D ** -0.5, 0.125, ((1, 8),)),
        "decay_log": draw_decay_log(jax.random.fold_in(keys[14], 71), 0),
        "init_state": normal_values(keys[6], (KEEPING_MIXERS, HEAD, HEAD), 4.0, 24.0, ((0, 8),)),
        "ret_gain": jnp.clip(1.0 + 0.18 * jax.random.normal(keys[7], (KEEPING_MIXERS * HEAD,), jnp.float32), 0.1, 1.9),
        "diff_query": draw_diff_query(jax.random.fold_in(keys[14], 71), 0),
        "diff_key": draw_diff_key(jax.random.fold_in(keys[14], 71), 0),
        "diff_value": normal_values(keys[10], (D, DIFF_HEADS * HEAD), D ** -0.5, 0.125, ((1, 8),)),
        "diff_lambda": jnp.clip(0.3 + 0.5 * jax.random.uniform(keys[11], (DIFF_HEADS,), jnp.float32) ** level_of(keys[11], (DIFF_HEADS,), ((0, 8),), -0.2, 0.2), 0.3, 0.8),
        "diff_gain": jnp.clip(1.0 + 0.18 * jax.random.normal(keys[12], (DIFF_HEADS * HEAD,), jnp.float32), 0.1, 1.9),
        "out_weight": normal_values(keys[13], (2, KEEPING_MIXERS * HEAD, D), (2 * KEEPING_MIXERS * HEAD) ** -0.5, 0.125, ((1, 8), (2, 4))),
    }


EPS = 1e-06
HUGE = 1e+30
UPPER_LIMIT = lax.Precision.HIGHEST

def norm_rows(rows, gain):
    widened = rows.astype(jnp.float32)
    fading_multiplier = lax.rsqrt(lax.optimization_barrier(jnp.mean(widened * widened, axis=-1, keepdims=True)) + EPS)
    return (widened * fading_multiplier * gain).astype(jnp.bfloat16)

def split_heads(normed, weight, width):
    result = jnp.dot(normed, weight, preferred_element_type=jnp.float32).astype(jnp.bfloat16)
    return jnp.transpose(result.reshape(1, TOKEN_COUNT, -1, width), (2, 0, 1, 3))

def group_norm(output, gain):
    centre = output - lax.optimization_barrier(jnp.mean(output, axis=-1, keepdims=True))
    fading_multiplier = lax.rsqrt(lax.optimization_barrier(jnp.mean(centre * centre, axis=-1, keepdims=True)) + EPS)
    return (centre * fading_multiplier * gain).astype(jnp.bfloat16)

def retention_head(query_rows, key_rows, value_rows, log_rates, start_state):
    seq_total = query_rows.shape[0]
    head_size = query_rows.shape[2]
    blocks = TOKEN_COUNT // RBLOCK

    def to_blocks(array):
        return jnp.swapaxes(array.reshape((seq_total, blocks, RBLOCK) + array.shape[2:]), 0, 1)
    lower = jnp.arange(RBLOCK)[:, None] >= jnp.arange(RBLOCK)[None, :]

    def advance(carried_state, inputs):
        block_queries, block_keys, block_values, block_rates = inputs
        cumulative_decay = jnp.cumsum(block_rates, axis=-1)
        gaps = jnp.where(lower, cumulative_decay[:, :, None] - cumulative_decay[:, None, :], -HUGE)
        widened_queries = block_queries.astype(jnp.float32)
        keys_wide = block_keys.astype(jnp.float32)
        widened_values = block_values.astype(jnp.float32)
        scores = jnp.einsum('sik,sjk->sij', widened_queries, keys_wide) * head_size ** (-0.5) * jnp.exp(gaps)
        rounded = lax.optimization_barrier(scores.astype(jnp.bfloat16)).astype(jnp.float32)
        inner = jnp.einsum('sij,sjv->siv', rounded, widened_values)
        reached_length = jnp.einsum('wny,wyo->wno', widened_queries * jnp.exp(cumulative_decay)[:, :, None], carried_state, precision=UPPER_LIMIT)
        ending_index = cumulative_decay[:, -1]
        weighted_values = keys_wide * (jnp.exp(ending_index[:, None] - cumulative_decay) * head_size ** (-0.5))[:, :, None]
        carried_state = jnp.exp(ending_index)[:, None, None] * carried_state + jnp.einsum('bdg,bdl->bgl', weighted_values, widened_values, precision=UPPER_LIMIT)
        return (carried_state, inner + reached_length)
    _, output = lax.scan(advance, start_state, (to_blocks(query_rows), to_blocks(key_rows), to_blocks(value_rows), to_blocks(log_rates)))
    return jnp.swapaxes(output, 0, 1).reshape(seq_total, TOKEN_COUNT, head_size)

def absorb(running, query_rows, key_rows, value_rows, allowed):
    peak_old, total_old, sum_old = running
    scores = jnp.einsum('...qd,...kd->...qk', query_rows.astype(jnp.float32), key_rows.astype(jnp.float32)) * query_rows.shape[-1] ** (-0.5)
    if allowed is not None:
        scores = jnp.where(allowed, scores, -HUGE)
    block_peak = lax.optimization_barrier(jnp.max(scores, axis=-1))
    weights = jnp.exp(scores - block_peak[..., None])
    block_total = lax.optimization_barrier(jnp.sum(weights, axis=-1))
    rounded = lax.optimization_barrier(weights.astype(jnp.bfloat16)).astype(jnp.float32)
    block_sum = jnp.einsum('...qk,...kv->...qv', rounded, value_rows.astype(jnp.float32))
    new_peak = jnp.maximum(peak_old, block_peak)
    before = jnp.exp(peak_old - new_peak)
    after = jnp.exp(block_peak - new_peak)
    return (new_peak, total_old * before + block_total * after, sum_old * before[..., None] + block_sum * after[..., None])

def diff_head(first_query, second_query, first_key, second_key, value_rows, lambda_head, gain):
    seq_total = first_query.shape[0]
    blocks = N_SP

    def as_blocks(array):
        return array.reshape(seq_total, blocks, SHARD_POSITIONS, array.shape[-1])
    within = jnp.arange(SHARD_POSITIONS)[:, None] >= jnp.arange(SHARD_POSITIONS)[None, :]
    queries = (as_blocks(first_query), as_blocks(second_query))
    key_sets = (as_blocks(first_key), as_blocks(second_key))
    values = as_blocks(value_rows)
    results = []
    for branch in range(2):
        running = (jnp.full((seq_total, blocks, SHARD_POSITIONS), -HUGE, jnp.float32), jnp.zeros((seq_total, blocks, SHARD_POSITIONS), jnp.float32), jnp.zeros((seq_total, blocks, SHARD_POSITIONS, values.shape[-1]), jnp.float32))
        for distance in range(blocks):
            allowed = within if distance == 0 else None
            fresh = absorb(tuple((member[:, distance:] for member in running)), queries[branch][:, distance:], key_sets[branch][:, :blocks - distance], values[:, :blocks - distance], allowed)
            running = tuple((member.at[:, distance:].set(update) for member, update in zip(running, fresh)))
        results.append(running)
    mixed = results[0][2] / results[0][1][..., None] - lambda_head * results[1][2] / results[1][1][..., None]
    mixed = mixed.reshape(seq_total, TOKEN_COUNT, -1)
    fading_multiplier = lax.rsqrt(lax.optimization_barrier(jnp.mean(mixed * mixed, axis=-1, keepdims=True)) + EPS)
    return (mixed * fading_multiplier * gain).astype(jnp.bfloat16)

def reference(tokens, in_gain, ret_query, ret_key, ret_value, decay_log, init_state, ret_gain, diff_query, diff_key, diff_value, diff_lambda, diff_gain, out_weight):
    normed = norm_rows(tokens, in_gain)
    ret_queries = split_heads(normed, ret_query, HEAD)
    ret_keys = split_heads(normed, ret_key, HEAD)
    ret_values = split_heads(normed, ret_value, HEAD)
    first_query = split_heads(normed, diff_query[0], MAP)
    second_query = split_heads(normed, diff_query[1], MAP)
    first_key = split_heads(normed, diff_key[0], MAP)
    second_key = split_heads(normed, diff_key[1], MAP)
    diff_values = split_heads(normed, diff_value, HEAD)
    rates = decay_log.reshape(KEEPING_MIXERS, 1, TOKEN_COUNT)
    starts = init_state.astype(jnp.float32).reshape(KEEPING_MIXERS, 1, HEAD, HEAD)

    def retention_item(head_items):
        output = retention_head(head_items[0], head_items[1], head_items[2], head_items[3], head_items[4])
        return group_norm(output, head_items[5])
    ret_mix = lax.map(retention_item, (ret_queries, ret_keys, ret_values, rates, starts, ret_gain.reshape(KEEPING_MIXERS, HEAD)))

    def diff_item(head_items):
        return diff_head(head_items[0], head_items[1], head_items[2], head_items[3], head_items[4], head_items[5], head_items[6])
    diff_mix = lax.map(diff_item, (first_query, second_query, first_key, second_key, diff_values, diff_lambda, diff_gain.reshape(DIFF_HEADS, HEAD)))
    ret_rows = out_weight[0].reshape(KEEPING_MIXERS, HEAD, D)
    diff_rows = out_weight[1].reshape(DIFF_HEADS, HEAD, D)

    def add_head(running_total, head_items):
        ret_part, diff_part, ret_weight, diff_weight = head_items
        partial_value = jnp.dot(ret_part.reshape(-1, HEAD), ret_weight, preferred_element_type=jnp.float32)
        partial_value = partial_value + jnp.dot(diff_part.reshape(-1, HEAD), diff_weight, preferred_element_type=jnp.float32)
        return (running_total + lax.optimization_barrier(partial_value.astype(jnp.bfloat16)).astype(jnp.float32), None)
    summed, _ = lax.scan(add_head, jnp.zeros((TOKEN_COUNT, D), jnp.float32), (ret_mix, diff_mix, ret_rows, diff_rows))
    return summed.astype(jnp.bfloat16)
```

```python
import jax
import jax.numpy as jnp
from jax import lax
from jax.sharding import PartitionSpec as P

RBLOCK = 128
EPS = 1e-06
HUGE = 1e30
HIGHEST = lax.Precision.HIGHEST
F32 = jnp.float32
BF16 = jnp.bfloat16


def dot(a, b, dims, **kw):
    return lax.dot_general(a, b, (dims, ((), ())), preferred_element_type=F32, **kw)


def nn(a, b, **kw):
    return dot(a, b, ((1,), (0,)), **kw)


def nt(a, b, **kw):
    return dot(a, b, ((1,), (1,)), **kw)


def tn(a, b, **kw):
    return dot(a, b, ((0,), (0,)), **kw)


def norm_rows(rows, gain):
    wide = rows.astype(F32)
    scale = lax.rsqrt(jnp.mean(wide * wide, axis=-1, keepdims=True) + EPS)
    return (wide * scale * gain).astype(BF16)


def few(count):
    return count in (2, 4)


def gathered_weight(out_weight, count):
    if few(count):
        blocks = [out_weight]
        for k in range(1, count):
            blocks.append(lax.ppermute(out_weight, "sp", [(i, i ^ k) for i in range(count)]))
        return blocks
    return [lax.all_gather(out_weight, "sp", axis=2, tiled=True)]


def earlier(packed, rows, head, place, count):
    if few(count):
        blocks = [lax.ppermute(packed, "sp", [(i, i + d) for i in range(count - d)]) for d in range(1, count)]
        pairs = [(b[:rows], b[rows : 2 * rows], place >= d) for d, b in enumerate(blocks, 1)]
        entering = jnp.zeros((head, head), F32)
        carry = jnp.ones((), F32)
        for d, block in enumerate(blocks, 1):
            entering = entering + carry * block[2 * rows : 2 * rows + head].astype(F32)
            carry = jnp.where(place >= d, carry * block[2 * rows + head, 0].astype(F32), carry)
        return pairs, entering, carry
    every = lax.all_gather(packed, "sp")
    keys = every[:, :rows].reshape(count * rows, -1)
    values = every[:, rows : 2 * rows].reshape(count * rows, -1)

    def step(b, state):
        entering, carry = state
        block = lax.dynamic_index_in_dim(every, b, 0, False)
        decay = block[2 * rows + head, 0].astype(F32)
        return decay * entering + block[2 * rows : 2 * rows + head].astype(F32), decay * carry

    entering, carry = lax.fori_loop(0, place, step, (jnp.zeros((head, head), F32), jnp.ones((), F32)))
    return [(keys, values, (jnp.arange(count * rows) < place * rows)[None, :])], entering, carry


def local(
    tokens, in_gain, ret_query, ret_key, ret_value, decay_log, init_state, ret_gain,
    diff_query, diff_key, diff_value, diff_lambda, diff_gain, out_weight,
):
    head = ret_query.shape[1]
    width = tokens.shape[1]
    count = lax.axis_size("sp")
    place = lax.axis_index("sp")
    group = lax.axis_size(("fs", "tp"))
    own_rows = tokens.shape[0]
    rows = own_rows * group

    weights = gathered_weight(out_weight, count)

    normed = norm_rows(lax.all_gather(tokens, ("fs", "tp"), axis=0, tiled=True), in_gain)
    ret_k = nn(normed, ret_key).astype(BF16)
    ret_v = nn(normed, ret_value).astype(BF16)
    keys = [nn(normed, diff_key[m]).astype(BF16) for m in range(2)]
    diff_v = nn(normed, diff_value).astype(BF16)
    lower = jnp.arange(rows)[:, None] >= jnp.arange(rows)[None, :]
    cumul = dot(lower.astype(F32), decay_log, ((1,), (1,)), precision=HIGHEST)
    last = cumul[-1:, :]
    key_weights = jnp.exp(last - cumul) * head ** (-0.5)
    state = tn(ret_k.astype(F32) * key_weights, ret_v.astype(F32), precision=HIGHEST)
    decay = jnp.exp(last)
    packed = jnp.concatenate(
        [jnp.concatenate(keys, axis=1), diff_v, state.astype(BF16), jnp.broadcast_to(decay, (8, head)).astype(BF16)], axis=0
    )
    received, entering, carry = earlier(packed, rows, head, place, count)

    ret_q = nn(normed, ret_query).astype(BF16)
    queries = [nn(normed, diff_query[m]).astype(BF16) for m in range(2)]
    row_cumul = cumul.reshape(1, rows)
    gaps = jnp.where(lower, cumul - row_cumul, -HUGE)
    scores = nt(ret_q, ret_k) * head ** (-0.5) * jnp.exp(gaps)
    inner = nn(scores.astype(BF16), ret_v)
    scaled = ret_q.astype(F32) * jnp.exp(cumul)
    entering = entering + carry * init_state[0].astype(F32)
    ret_out = inner + nn(scaled, entering, precision=HIGHEST)
    centre = ret_out - jnp.mean(ret_out, axis=-1, keepdims=True)
    ret_mix = (centre * lax.rsqrt(jnp.mean(centre * centre, axis=-1, keepdims=True) + EPS) * ret_gain).astype(BF16)

    maps = []
    half = keys[0].shape[1]
    for m in range(2):
        parts = [jnp.where(lower, nt(queries[m], keys[m]) * half ** (-0.5), -HUGE)]
        for block_keys, _, allowed in received:
            s = nt(queries[m], block_keys[:, m * half : (m + 1) * half]) * half ** (-0.5)
            parts.append(jnp.where(allowed, s, -HUGE))
        top = parts[0].max(axis=-1, keepdims=True)
        for part in parts[1:]:
            top = jnp.maximum(top, part.max(axis=-1, keepdims=True))
        total, sums = 0.0, 0.0
        for part, value in zip(parts, [diff_v] + [values for _, values, _ in received]):
            e = jnp.exp(part - top)
            total = total + e.sum(axis=-1, keepdims=True)
            sums = sums + nn(e.astype(BF16), value)
        maps.append(sums / total)
    diff_out = maps[0] - diff_lambda[0] * maps[1]
    diff_mix = (diff_out * lax.rsqrt(jnp.mean(diff_out * diff_out, axis=-1, keepdims=True) + EPS) * diff_gain).astype(BF16)

    mixed = jnp.concatenate([ret_mix, diff_mix], axis=1)
    partial = jnp.stack([nn(mixed, w.reshape(2 * head, -1)).astype(BF16) for w in weights], axis=1)
    shares = lax.all_to_all(partial, ("fs", "tp"), 0, 0, tiled=True)
    summed = shares.reshape((group, own_rows) + partial.shape[1:]).astype(F32).sum(axis=0).astype(BF16)
    if few(count):
        summed = jnp.stack([lax.dynamic_index_in_dim(summed, c ^ place, 1, False) for c in range(count)], axis=1)
    return summed.reshape(own_rows, width)


def solution(mesh):
    in_specs = (
        P(("sp", "fs", "tp"), None),
        P(),
        P(None, ("fs", "tp")),
        P(None, ("fs", "tp")),
        P(None, ("fs", "tp")),
        P(("fs", "tp"), "sp"),
        P(("fs", "tp"), None, None),
        P(("fs", "tp")),
        P(None, None, ("fs", "tp")),
        P(None, None, ("fs", "tp")),
        P(None, ("fs", "tp")),
        P(("fs", "tp")),
        P(("fs", "tp")),
        P(None, ("fs", "tp"), "sp"),
    )
    out_specs = P(("sp", "fs", "tp"), None)
    return jax.shard_map(local, mesh=mesh, in_specs=in_specs, out_specs=out_specs, check_vma=False)
```

```python
import jax
import jax.numpy as jnp
from jax import lax
from jax.experimental import pallas as pl
from jax.experimental.pallas import tpu as pltpu
from jax.sharding import PartitionSpec as P


EPS = 1e-06
HUGE = 1e30
HIGHEST = lax.Precision.HIGHEST
F32 = jnp.float32
BF16 = jnp.bfloat16


def dot(a, b, dims, **kw):
    return lax.dot_general(a, b, (dims, ((), ())), preferred_element_type=F32, **kw)


def nn(a, b, **kw):
    return dot(a, b, ((1,), (0,)), **kw)


def nt(a, b, **kw):
    return dot(a, b, ((1,), (1,)), **kw)


def tn(a, b, **kw):
    return dot(a, b, ((0,), (0,)), **kw)


def few(count):
    return count in (2, 4)


def at_or_before(n):
    return lax.broadcasted_iota(jnp.int32, (n, n), 1) <= lax.broadcasted_iota(jnp.int32, (n, n), 0)


def cumulated(decay_row):
    n = decay_row.shape[1]
    row = lax.broadcasted_iota(jnp.int32, (n, n), 0)
    col = lax.broadcasted_iota(jnp.int32, (n, n), 1)
    wide = jnp.broadcast_to(decay_row, (n, n))
    down = jnp.sum(jnp.where(col <= row, wide, 0.0), axis=1, keepdims=True)
    decay_col = jnp.sum(jnp.where(col == row, wide, 0.0), axis=1, keepdims=True)
    along = jnp.sum(jnp.where(row <= col, decay_col, 0.0), axis=0, keepdims=True)
    return down, along


def project_kernel(x, gain, wk, wv, dk, dv, decay, normed, packed, ret_k, ret_v):
    rows, head = ret_k.shape
    wide = x[...].astype(F32)
    scale = lax.rsqrt(jnp.mean(wide * wide, axis=-1, keepdims=True) + EPS)
    rounded = (wide * scale * gain[...]).astype(BF16)
    normed[...] = rounded
    k = nn(rounded, wk[...]).astype(BF16)
    v = nn(rounded, wv[...]).astype(BF16)
    ret_k[...] = k
    ret_v[...] = v
    cumul, _ = cumulated(decay[...])
    last = cumul[rows - 1 :, :]
    weighted = k.astype(F32) * (jnp.exp(last - cumul) * head ** (-0.5))
    state = tn(weighted, v.astype(F32), precision=HIGHEST)
    keys = nt(rounded, dk[...].reshape(-1, dk.shape[2]))
    packed[0:rows, :] = keys.astype(BF16)
    packed[rows : 2 * rows, :] = nn(rounded, dv[...]).astype(BF16)
    packed[2 * rows : 2 * rows + head, :] = state.astype(BF16)
    factor = jnp.broadcast_to(jnp.exp(last), (8, head))
    packed[2 * rows + head :, :] = factor.astype(BF16)


def own_kernel(normed, wq, dq, packed, ret_k, ret_v, decay, lam, init, queries, scaled, inner, sums, stats):
    rows, head = ret_k.shape
    x = normed[...]
    q = nn(x, wq[...]).astype(BF16)
    cumul, along = cumulated(decay[...])
    lower = at_or_before(rows)
    weights = nt(q, ret_k[...]) * head ** (-0.5) * jnp.exp(jnp.where(lower, cumul - along, -HUGE))
    inner[...] = nn(weights.astype(BF16), ret_v[...])
    scaled[...] = q.astype(F32) * jnp.exp(cumul)
    both = nt(x, dq[...].reshape(-1, dq.shape[2])).astype(BF16)
    queries[...] = both
    half = head // 2
    keys = packed[0:rows, :]
    values = packed[rows : 2 * rows, :]
    for m in range(2):
        s = nt(both[:, m * half : (m + 1) * half], keys[:, m * half : (m + 1) * half]) * half ** (-0.5)
        s = jnp.where(lower, s, -HUGE)
        top = jnp.max(s, axis=-1, keepdims=True)
        e = jnp.exp(s - top)
        sums[m] = nn(e.astype(BF16), values)
        stats[m] = jnp.concatenate([jnp.broadcast_to(top, (rows, half)), jnp.broadcast_to(jnp.sum(e, axis=-1, keepdims=True), (rows, half))], axis=1)


def finish_kernel(count, *refs):
    queries, scaled, inner, sums, stats, lam, init, ret_gain, diff_gain = refs[:9]
    blocks = refs[9 : 8 + count]
    weights = refs[8 + count : 8 + 2 * count]
    partial = refs[8 + 2 * count]
    rows, head = inner.shape
    half = head // 2
    place = lax.axis_index("sp")
    entering = jnp.zeros((head, head), F32)
    carry = jnp.ones((1, head), F32)
    for d, block in enumerate(blocks, 1):
        entering = entering + carry * block[2 * rows : 2 * rows + head, :].astype(F32)
        factor = block[2 * rows + head : 2 * rows + head + 8, :].astype(F32)[0:1, :]
        carry = jnp.where(place >= d, carry * factor, carry)
    entering = entering + carry * init[0].astype(F32)
    ret_out = inner[...] + nn(scaled[...], entering, precision=HIGHEST)
    centre = ret_out - jnp.mean(ret_out, axis=-1, keepdims=True)
    spread = lax.rsqrt(jnp.mean(centre * centre, axis=-1, keepdims=True) + EPS)
    ret_mix = (centre * spread * ret_gain[...]).astype(BF16)

    keys = jnp.concatenate([b[0:rows, :] for b in blocks], axis=0)
    values = jnp.concatenate([b[rows : 2 * rows, :] for b in blocks], axis=0)
    distance = 1 + lax.broadcasted_iota(jnp.int32, (1, keys.shape[0]), 1) // rows
    allowed = distance <= place
    maps = []
    for m in range(2):
        s = nt(queries[:, m * half : (m + 1) * half], keys[:, m * half : (m + 1) * half]) * half ** (-0.5)
        s = jnp.where(allowed, s, -HUGE)
        old_top = stats[m][:, 0:1]
        old_total = stats[m][:, half : half + 1]
        top = jnp.maximum(old_top, jnp.max(s, axis=-1, keepdims=True))
        e = jnp.exp(s - top)
        keep = jnp.exp(old_top - top)
        total = old_total * keep + jnp.sum(e, axis=-1, keepdims=True)
        maps.append((sums[m] * keep + nn(e.astype(BF16), values)) / total)
    diff_out = maps[0] - lam[0] * maps[1]
    level = lax.rsqrt(jnp.mean(diff_out * diff_out, axis=-1, keepdims=True) + EPS)
    diff_mix = (diff_out * level * diff_gain[...]).astype(BF16)

    mixed = jnp.concatenate([ret_mix, diff_mix], axis=1)
    for k, w in enumerate(weights):
        cols = w.shape[2]
        at = pl.multiple_of((place ^ k) * cols, cols)
        partial[:, pl.ds(at, cols)] = nn(mixed, w[...].reshape(2 * head, cols)).astype(BF16)


def call(kernel, outs, flops, smem=(), n=0):
    specs = [pl.BlockSpec(memory_space=pltpu.SMEM if i in smem else pltpu.VMEM) for i in range(n)]
    return pl.pallas_call(
        kernel,
        out_shape=outs,
        in_specs=specs,
        out_specs=[pl.BlockSpec(memory_space=pltpu.VMEM)] * len(outs),
        compiler_params=pltpu.CompilerParams(vmem_limit_bytes=24 * 1024 * 1024),
        cost_estimate=pl.CostEstimate(flops=flops, bytes_accessed=1 << 20, transcendentals=1 << 16),
    )


def shape(dims, kind):
    return jax.ShapeDtypeStruct(dims, kind)


def local_few(
    tokens, in_gain, ret_query, ret_key, ret_value, decay_log, init_state, ret_gain,
    diff_query, diff_key, diff_value, diff_lambda, diff_gain, out_weight,
):
    head = ret_query.shape[1]
    width = tokens.shape[1]
    count = lax.axis_size("sp")
    group = lax.axis_size(("fs", "tp"))
    own_rows = tokens.shape[0]
    rows = own_rows * group

    def swapped(array, k):
        return lax.ppermute(array, "sp", [(i, i ^ k) for i in range(count)])

    weights = [out_weight] * count
    weights[1] = swapped(out_weight, 1)
    if count == 4:
        weights[2] = swapped(out_weight, 2)
        weights[3] = swapped(weights[2], 1)
    gathered = lax.all_gather(tokens, ("fs", "tp"), axis=0, tiled=True)
    square = shape((rows, head), BF16)
    normed, packed, ret_k, ret_v = call(
        project_kernel, [shape((rows, width), BF16), shape((2 * rows + head + 8, head), BF16), square, square],
        flops=2 * rows * width * head * 4, n=7,
    )(gathered, in_gain[None, :], ret_key, ret_value, jnp.swapaxes(diff_key, 1, 2), diff_value, decay_log)
    blocks = []
    for d in range(1, count):
        blocks.append(lax.ppermute(packed, "sp", [(i, i + d) for i in range(count - d)]))
    wide = shape((rows, head), F32)
    pair = shape((2, rows, head), F32)
    mine = call(
        own_kernel, [square, wide, wide, pair, pair], flops=2 * rows * width * head * 2, smem=(7,), n=9,
    )(normed, ret_query, jnp.swapaxes(diff_query, 1, 2), packed, ret_k, ret_v, decay_log, diff_lambda, init_state)
    (partial,) = call(
        lambda *refs: finish_kernel(count, *refs), [shape((rows, width), BF16)],
        flops=2 * rows * width * head * 2, smem=(5,), n=8 + 2 * count,
    )(*mine, diff_lambda, init_state, ret_gain[None, :], diff_gain[None, :], *blocks, *weights)
    shares = lax.all_to_all(partial, ("fs", "tp"), 0, 0, tiled=True)
    return shares.reshape(group, own_rows, width).astype(F32).sum(axis=0).astype(BF16)


def local_many(
    tokens, in_gain, ret_query, ret_key, ret_value, decay_log, init_state, ret_gain,
    diff_query, diff_key, diff_value, diff_lambda, diff_gain, out_weight,
):
    head = ret_query.shape[1]
    width = tokens.shape[1]
    count = lax.axis_size("sp")
    place = lax.axis_index("sp")
    group = lax.axis_size(("fs", "tp"))
    own_rows = tokens.shape[0]
    rows = own_rows * group

    full_weight = lax.all_gather(out_weight, "sp", axis=2, tiled=True).reshape(2 * head, width)
    wide = lax.all_gather(tokens, ("fs", "tp"), axis=0, tiled=True).astype(F32)
    normed = (wide * lax.rsqrt(jnp.mean(wide * wide, axis=-1, keepdims=True) + EPS) * in_gain).astype(BF16)
    ret_q, ret_k, ret_v, diff_v = (nn(normed, w).astype(BF16) for w in (ret_query, ret_key, ret_value, diff_value))
    queries = [nn(normed, diff_query[m]).astype(BF16) for m in range(2)]
    keys = [nn(normed, diff_key[m]).astype(BF16) for m in range(2)]
    lower = at_or_before(rows)
    cumul, along = cumulated(decay_log)
    last = cumul[-1:, :]
    weighted = ret_k.astype(F32) * (jnp.exp(last - cumul) * head ** (-0.5))
    state = tn(weighted, ret_v.astype(F32), precision=HIGHEST)
    factor = jnp.broadcast_to(jnp.exp(last), (8, head))
    packed = jnp.concatenate([jnp.concatenate(keys, axis=1), diff_v, state.astype(BF16), factor.astype(BF16)], axis=0)
    every = lax.all_gather(packed, "sp")
    all_keys = every[:, :rows].reshape(count * rows, -1)
    all_values = every[:, rows : 2 * rows].reshape(count * rows, -1)

    def step(b, carried):
        block = lax.dynamic_index_in_dim(every, b, 0, False).astype(F32)
        return block[2 * rows + head, 0] * carried + block[2 * rows : 2 * rows + head]

    entering = lax.fori_loop(0, place, step, init_state[0].astype(F32))
    scores = nt(ret_q, ret_k) * head ** (-0.5) * jnp.exp(jnp.where(lower, cumul - along, -HUGE))
    ret_out = nn(scores.astype(BF16), ret_v) + nn(ret_q.astype(F32) * jnp.exp(cumul), entering, precision=HIGHEST)
    centre = ret_out - jnp.mean(ret_out, axis=-1, keepdims=True)
    ret_mix = (centre * lax.rsqrt(jnp.mean(centre * centre, axis=-1, keepdims=True) + EPS) * ret_gain).astype(BF16)

    maps = []
    half = head // 2
    allowed = jnp.arange(count * rows)[None, :] <= (place * rows + jnp.arange(rows))[:, None]
    for m in range(2):
        s = nt(queries[m], all_keys[:, m * half : (m + 1) * half]) * half ** (-0.5)
        s = jnp.where(allowed, s, -HUGE)
        e = jnp.exp(s - s.max(axis=-1, keepdims=True))
        maps.append(nn(e.astype(BF16), all_values) / e.sum(axis=-1, keepdims=True))
    diff_out = maps[0] - diff_lambda[0] * maps[1]
    level = lax.rsqrt(jnp.mean(diff_out * diff_out, axis=-1, keepdims=True) + EPS)
    diff_mix = (diff_out * level * diff_gain).astype(BF16)

    mixed = jnp.concatenate([ret_mix, diff_mix], axis=1)
    partial = nn(mixed, full_weight).astype(BF16)
    shares = lax.all_to_all(partial, ("fs", "tp"), 0, 0, tiled=True)
    return shares.reshape(group, own_rows, width).astype(F32).sum(axis=0).astype(BF16)


def solution(mesh):
    count = mesh.shape["sp"]
    in_specs = (
        P(("sp", "fs", "tp"), None),
        P(),
        P(None, ("fs", "tp")),
        P(None, ("fs", "tp")),
        P(None, ("fs", "tp")),
        P(("fs", "tp"), "sp"),
        P(("fs", "tp"), None, None),
        P(("fs", "tp")),
        P(None, None, ("fs", "tp")),
        P(None, None, ("fs", "tp")),
        P(None, ("fs", "tp")),
        P(("fs", "tp")),
        P(("fs", "tp")),
        P(None, ("fs", "tp"), "sp"),
    )
    out_specs = P(("sp", "fs", "tp"), None)
    local = local_few if few(count) else local_many
    return jax.shard_map(local, mesh=mesh, in_specs=in_specs, out_specs=out_specs, check_vma=False)
```

```python
import functools

import jax
import jax.numpy as jnp
from jax import lax
from jax.experimental import pallas as pl
from jax.experimental.pallas import tpu as pltpu
from jax.sharding import PartitionSpec as P


EPS = 1e-06
HUGE = 1e30
HIGHEST = lax.Precision.HIGHEST
F32 = jnp.float32
BF16 = jnp.bfloat16

GATHER_FLOPS = 10**10


def dot(a, b, dims, **kw):
    return lax.dot_general(a, b, (dims, ((), ())), preferred_element_type=F32, **kw)


def nn(a, b, **kw):
    return dot(a, b, ((1,), (0,)), **kw)


def nt(a, b, **kw):
    return dot(a, b, ((1,), (1,)), **kw)


def tn(a, b, **kw):
    return dot(a, b, ((0,), (0,)), **kw)


def route(d, count):
    return [(i, i + d) for i in range(count - d)], lambda at: at - d


def few(count):
    return count in (2, 4)


def at_or_before(n):
    return lax.broadcasted_iota(jnp.int32, (n, n), 1) <= lax.broadcasted_iota(jnp.int32, (n, n), 0)


def cumulated(decay_row):
    n = decay_row.shape[1]
    row = lax.broadcasted_iota(jnp.int32, (n, n), 0)
    col = lax.broadcasted_iota(jnp.int32, (n, n), 1)
    wide = jnp.broadcast_to(decay_row, (n, n))
    down = jnp.sum(jnp.where(col <= row, wide, 0.0), axis=1, keepdims=True)
    decay_col = jnp.sum(jnp.where(col == row, wide, 0.0), axis=1, keepdims=True)
    along = jnp.sum(jnp.where(row <= col, decay_col, 0.0), axis=0, keepdims=True)
    return down, along


def fetch(pairs, sems):
    copies = [pltpu.make_async_copy(src, dst, sems.at[i]) for i, (src, dst) in enumerate(pairs)]
    for copy in copies:
        copy.start()
    return copies


def prepare_kernel(
    tokens_h, decay_h, in_gain_h, ret_gain_h, diff_gain_h, init_h,
    tokens, key_scale, query_scale, fade, factor, in_gain, small, init, decay, ret_gain, diff_gain, start, sems,
):
    head = fade.shape[0]
    copies = fetch(
        [(decay_h, decay), (tokens_h, tokens), (in_gain_h, in_gain), (ret_gain_h, ret_gain), (diff_gain_h, diff_gain), (init_h, start)],
        sems,
    )
    copies[0].wait()
    cumul, along = cumulated(decay[...])
    rows = cumul.shape[0]
    last = cumul[rows - 1 :, :]
    key_scale[...] = jnp.broadcast_to(jnp.exp(last - cumul) * head ** (-0.5), (rows, head))
    query_scale[...] = jnp.broadcast_to(jnp.exp(cumul), (rows, head))
    fade[...] = jnp.exp(jnp.where(at_or_before(rows), cumul - along, -HUGE)) * head ** (-0.5)
    factor[...] = jnp.broadcast_to(jnp.exp(last), (8, head))
    for copy in copies[1:]:
        copy.wait()
    small[0:8, :] = jnp.broadcast_to(ret_gain[...], (8, head))
    small[8:16, :] = jnp.broadcast_to(diff_gain[...], (8, head))
    init[...] = start[0].astype(F32)


def project_kernel(x, gain, key_scale, factor, dk, dv, wk, wv, normed, packed, ret_k, ret_v):
    rows, head = ret_k.shape
    wide = x[...].astype(F32)
    scale = lax.rsqrt(jnp.mean(wide * wide, axis=-1, keepdims=True) + EPS)
    rounded = (wide * scale * gain[...]).astype(BF16)
    normed[...] = rounded
    packed[0:rows, :] = nt(rounded, dk[...].reshape(-1, dk.shape[2])).astype(BF16)
    packed[rows : 2 * rows, :] = nn(rounded, dv[...]).astype(BF16)
    k = nn(rounded, wk[...]).astype(BF16)
    v = nn(rounded, wv[...]).astype(BF16)
    ret_k[...] = k
    ret_v[...] = v
    state = tn(k.astype(F32) * key_scale[...], v.astype(F32), precision=HIGHEST)
    packed[2 * rows : 2 * rows + head, :] = state.astype(BF16)
    packed[2 * rows + head :, :] = factor[...].astype(BF16)


def own_kernel(lam, normed, packed, ret_k, ret_v, query_scale, fade, wq, dq, queries, scaled, inner, sums, stats, second):
    rows, head = ret_k.shape
    second[...] = jnp.full(second.shape, lam[0])
    x = normed[...]
    q = nn(x, wq[...]).astype(BF16)
    weights = nt(q, ret_k[...]) * fade[...]
    inner[...] = nn(weights.astype(BF16), ret_v[...])
    scaled[...] = q.astype(F32) * query_scale[...]
    both = nt(x, dq[...].reshape(-1, dq.shape[2])).astype(BF16)
    queries[...] = both
    half = head // 2
    lower = at_or_before(rows)
    keys = packed[0:rows, :]
    values = packed[rows : 2 * rows, :]
    for m in range(2):
        s = nt(both[:, m * half : (m + 1) * half], keys[:, m * half : (m + 1) * half]) * half ** (-0.5)
        s = jnp.where(lower, s, -HUGE)
        top = jnp.max(s, axis=-1, keepdims=True)
        e = jnp.exp(s - top)
        sums[m] = nn(e.astype(BF16), values)
        stats[m] = jnp.concatenate([jnp.broadcast_to(top, (rows, half)), jnp.broadcast_to(jnp.sum(e, axis=-1, keepdims=True), (rows, half))], axis=1)


def finish_kernel(sources, *refs):
    count = len(sources) + 1
    queries, scaled, inner, sums, stats, second, small, init = refs[:8]
    blocks = refs[8 : 7 + count]
    weights = refs[7 + count : 7 + 2 * count]
    keep, send, mixed = refs[7 + 2 * count :]
    rows, head = inner.shape
    half = head // 2
    place = lax.axis_index("sp")
    core = lax.axis_index("tp")
    source = [f(place) for f in sources]
    before = [jnp.logical_and(at >= 0, at < place) for at in source]
    factors = [b[2 * rows + head : 2 * rows + head + 8, :].astype(F32)[0:1, :] for b in blocks]
    entering = init[...]
    for factor, here in zip(factors, before):
        entering = entering * jnp.where(here, factor, 1.0)
    for j, block in enumerate(blocks):
        carry = jnp.where(before[j], 1.0, 0.0) * jnp.ones((1, head), F32)
        for i, factor in enumerate(factors):
            if i != j:
                carry = carry * jnp.where(jnp.logical_and(source[i] > source[j], before[i]), factor, 1.0)
        entering = entering + carry * block[2 * rows : 2 * rows + head, :].astype(F32)
    ret_out = inner[...] + nn(scaled[...], entering, precision=HIGHEST)
    centre = ret_out - jnp.mean(ret_out, axis=-1, keepdims=True)
    spread = lax.rsqrt(jnp.mean(centre * centre, axis=-1, keepdims=True) + EPS)
    ret_mix = (centre * spread * small[0:1, :]).astype(BF16)

    keys = jnp.concatenate([b[0:rows, :] for b in blocks], axis=0)
    values = jnp.concatenate([b[rows : 2 * rows, :] for b in blocks], axis=0)
    allowed = jnp.concatenate([jnp.full((1, rows), jnp.where(here, 1, 0)) for here in before], axis=1) > 0
    maps = []
    for m in range(2):
        s = nt(queries[:, m * half : (m + 1) * half], keys[:, m * half : (m + 1) * half]) * half ** (-0.5)
        s = jnp.where(allowed, s, -HUGE)
        old_top = stats[m][:, 0:1]
        old_total = stats[m][:, half : half + 1]
        top = jnp.maximum(old_top, jnp.max(s, axis=-1, keepdims=True))
        e = jnp.exp(s - top)
        kept = jnp.exp(old_top - top)
        total = old_total * kept + jnp.sum(e, axis=-1, keepdims=True)
        maps.append((sums[m] * kept + nn(e.astype(BF16), values)) / total)
    diff_out = maps[0] - second[0:1, :] * maps[1]
    level = lax.rsqrt(jnp.mean(diff_out * diff_out, axis=-1, keepdims=True) + EPS)
    diff_mix = (diff_out * level * small[8:9, :]).astype(BF16)

    mixed[:, :, :, :head] = ret_mix.reshape(mixed.shape[:3] + (head,))
    mixed[:, :, :, head:] = diff_mix.reshape(mixed.shape[:3] + (head,))
    ordered = jnp.concatenate([mixed[:, core].reshape(-1, 2 * head), mixed[:, 1 - core].reshape(-1, 2 * head)], axis=0)
    for k, w in enumerate(weights):
        cols = w.shape[2]
        at = pl.ds(pl.multiple_of((place ^ k) * cols, cols), cols)
        result = nn(ordered, w[...].reshape(2 * head, cols))
        keep[:, at] = result[: rows // 2]
        send[:, at] = result[rows // 2 :].astype(BF16)


def call(kernel, outs, flops, here, away=0, scratch=(), scalars=0):
    spots = [pltpu.SMEM] * scalars + [pltpu.VMEM] * here + [pltpu.HBM] * away
    run = pl.pallas_call(
        kernel,
        out_shape=outs,
        in_specs=[pl.BlockSpec(memory_space=spot) for spot in spots],
        out_specs=[pl.BlockSpec(memory_space=pltpu.VMEM)] * len(outs),
        scratch_shapes=list(scratch) + ([pltpu.SemaphoreType.DMA((away,))] if away else []),
        compiler_params=pltpu.CompilerParams(vmem_limit_bytes=24 * 1024 * 1024),
        cost_estimate=pl.CostEstimate(flops=flops, bytes_accessed=1 << 20, transcendentals=1 << 16),
    )

    def placed(*args):
        return run(*[a if spot is pltpu.SMEM else pltpu.with_memory_space_constraint(a, spot) for a, spot in zip(args, spots)])

    return placed


def shape(dims, kind):
    return pltpu.VMEM(dims, kind)


def local_few(
    tokens, in_gain, ret_query, ret_key, ret_value, decay_log, init_state, ret_gain,
    diff_query, diff_key, diff_value, diff_lambda, diff_gain, out_weight,
):
    head = ret_query.shape[1]
    width = tokens.shape[1]
    count = lax.axis_size("sp")
    group = lax.axis_size(("fs", "tp"))
    own_rows = tokens.shape[0]
    rows = own_rows * group

    def swapped(array, k):
        return lax.ppermute(array, "sp", [(i, i ^ k) for i in range(count)])

    weights = [out_weight] * count
    weights[1] = swapped(out_weight, 1)
    if count == 4:
        weights[2] = swapped(out_weight, 2)
        weights[3] = swapped(weights[2], 1)
    square = shape((rows, head), BF16)
    wide = shape((rows, head), F32)
    line = pltpu.VMEM((1, head), F32)
    staged, key_scale, query_scale, fade, factor, gain, small, init = call(
        prepare_kernel,
        [shape(tokens.shape, BF16), wide, wide, shape((rows, rows), F32), shape((8, head), F32),
         shape((1, width), F32), shape((16, head), F32), shape((head, head), F32)],
        GATHER_FLOPS, 0, 6, [line, line, line, pltpu.VMEM((1, head, head), BF16)],
    )(tokens, decay_log, in_gain[None, :], ret_gain[None, :], diff_gain[None, :], init_state)
    gathered = lax.all_gather(staged, ("fs", "tp"), axis=0, tiled=True)
    normed, packed, ret_k, ret_v = call(
        project_kernel, [shape((rows, width), BF16), shape((2 * rows + head + 8, head), BF16), square, square],
        2 * rows * width * head * 4, 8,
    )(gathered, gain, key_scale, factor, jnp.swapaxes(diff_key, 1, 2), diff_value, ret_key, ret_value)
    blocks, sources = [], []
    for d in range(1, count):
        pairs, source = route(d, count)
        sources.append(source)
        blocks.append(lax.ppermute(packed, "sp", pairs))
    pair = shape((2, rows, head), F32)
    mine = call(own_kernel, [square, wide, wide, pair, pair, shape((8, head), F32)], 2 * rows * width * head * 2, 8, scalars=1)(
        diff_lambda, normed, packed, ret_k, ret_v, query_scale, fade, ret_query, jnp.swapaxes(diff_query, 1, 2)
    )
    cores = lax.axis_size("tp")
    keep, send = call(
        functools.partial(finish_kernel, sources), [shape((rows // 2, width), F32), shape((rows // 2, width), BF16)],
        2 * rows * width * head * 2, 7 + 2 * count,
        scratch=[pltpu.VMEM((group // cores, cores, own_rows, 2 * head), BF16)],
    )(*mine, small, init, *blocks, *weights)
    other = lax.ppermute(send, "tp", [(0, 1), (1, 0)])
    both = (keep + other.astype(F32)).astype(BF16)
    shares = lax.all_to_all(both, "fs", 0, 0, tiled=True)
    return shares.reshape(group // cores, own_rows, width).astype(F32).sum(axis=0).astype(BF16)


def local_many(
    tokens, in_gain, ret_query, ret_key, ret_value, decay_log, init_state, ret_gain,
    diff_query, diff_key, diff_value, diff_lambda, diff_gain, out_weight,
):
    head = ret_query.shape[1]
    width = tokens.shape[1]
    count = lax.axis_size("sp")
    place = lax.axis_index("sp")
    group = lax.axis_size(("fs", "tp"))
    own_rows = tokens.shape[0]
    rows = own_rows * group

    full_weight = lax.all_gather(out_weight, "sp", axis=2, tiled=True).reshape(2 * head, width)
    wide = lax.all_gather(tokens, ("fs", "tp"), axis=0, tiled=True).astype(F32)
    normed = (wide * lax.rsqrt(jnp.mean(wide * wide, axis=-1, keepdims=True) + EPS) * in_gain).astype(BF16)
    ret_q, ret_k, ret_v, diff_v = (nn(normed, w).astype(BF16) for w in (ret_query, ret_key, ret_value, diff_value))
    queries = [nn(normed, diff_query[m]).astype(BF16) for m in range(2)]
    keys = [nn(normed, diff_key[m]).astype(BF16) for m in range(2)]
    lower = at_or_before(rows)
    cumul, along = cumulated(decay_log)
    last = cumul[-1:, :]
    weighted = ret_k.astype(F32) * (jnp.exp(last - cumul) * head ** (-0.5))
    state = tn(weighted, ret_v.astype(F32), precision=HIGHEST)
    factor = jnp.broadcast_to(jnp.exp(last), (8, head))
    packed = jnp.concatenate([jnp.concatenate(keys, axis=1), diff_v, state.astype(BF16), factor.astype(BF16)], axis=0)
    every = lax.all_gather(packed, "sp")
    all_keys = every[:, :rows].reshape(count * rows, -1)
    all_values = every[:, rows : 2 * rows].reshape(count * rows, -1)

    def step(b, carried):
        block = lax.dynamic_index_in_dim(every, b, 0, False).astype(F32)
        return block[2 * rows + head, 0] * carried + block[2 * rows : 2 * rows + head]

    entering = lax.fori_loop(0, place, step, init_state[0].astype(F32))
    scores = nt(ret_q, ret_k) * head ** (-0.5) * jnp.exp(jnp.where(lower, cumul - along, -HUGE))
    ret_out = nn(scores.astype(BF16), ret_v) + nn(ret_q.astype(F32) * jnp.exp(cumul), entering, precision=HIGHEST)
    centre = ret_out - jnp.mean(ret_out, axis=-1, keepdims=True)
    ret_mix = (centre * lax.rsqrt(jnp.mean(centre * centre, axis=-1, keepdims=True) + EPS) * ret_gain).astype(BF16)

    maps = []
    half = head // 2
    allowed = jnp.arange(count * rows)[None, :] <= (place * rows + jnp.arange(rows))[:, None]
    for m in range(2):
        s = nt(queries[m], all_keys[:, m * half : (m + 1) * half]) * half ** (-0.5)
        s = jnp.where(allowed, s, -HUGE)
        e = jnp.exp(s - s.max(axis=-1, keepdims=True))
        maps.append(nn(e.astype(BF16), all_values) / e.sum(axis=-1, keepdims=True))
    diff_out = maps[0] - diff_lambda[0] * maps[1]
    level = lax.rsqrt(jnp.mean(diff_out * diff_out, axis=-1, keepdims=True) + EPS)
    diff_mix = (diff_out * level * diff_gain).astype(BF16)

    mixed = jnp.concatenate([ret_mix, diff_mix], axis=1)
    partial = nn(mixed, full_weight).astype(BF16)
    shares = lax.all_to_all(partial, ("fs", "tp"), 0, 0, tiled=True)
    return shares.reshape(group, own_rows, width).astype(F32).sum(axis=0).astype(BF16)


def solution(mesh):
    count = mesh.shape["sp"]
    in_specs = (
        P(("sp", "fs", "tp"), None),
        P(),
        P(None, ("fs", "tp")),
        P(None, ("fs", "tp")),
        P(None, ("fs", "tp")),
        P(("fs", "tp"), "sp"),
        P(("fs", "tp"), None, None),
        P(("fs", "tp")),
        P(None, None, ("fs", "tp")),
        P(None, None, ("fs", "tp")),
        P(None, ("fs", "tp")),
        P(("fs", "tp")),
        P(("fs", "tp")),
        P(None, ("fs", "tp"), "sp"),
    )
    out_specs = P(("sp", "fs", "tp"), None)
    local = local_few if few(count) and mesh.shape["tp"] == 2 else local_many
    return jax.shard_map(local, mesh=mesh, in_specs=in_specs, out_specs=out_specs, check_vma=False)
```

```python
import functools

import jax
import jax.numpy as jnp
from jax import lax
from jax.experimental import pallas as pl
from jax.experimental.pallas import tpu as pltpu
from jax.sharding import PartitionSpec as P


EPS = 1e-06
HUGE = 1e30
HIGHEST = lax.Precision.HIGHEST
F32 = jnp.float32
BF16 = jnp.bfloat16

GATHER_FLOPS = 3 * 10**10


def dot(a, b, dims, **kw):
    return lax.dot_general(a, b, (dims, ((), ())), preferred_element_type=F32, **kw)


def nn(a, b, **kw):
    return dot(a, b, ((1,), (0,)), **kw)


def nt(a, b, **kw):
    return dot(a, b, ((1,), (1,)), **kw)


def tn(a, b, **kw):
    return dot(a, b, ((0,), (0,)), **kw)


def route(d, count):
    return [(i, i + d) for i in range(count - d)], lambda at: at - d


def few(count):
    return count in (2, 4)


def at_or_before(n):
    return lax.broadcasted_iota(jnp.int32, (n, n), 1) <= lax.broadcasted_iota(jnp.int32, (n, n), 0)


def cumulated(decay_row):
    n = decay_row.shape[1]
    row = lax.broadcasted_iota(jnp.int32, (n, n), 0)
    col = lax.broadcasted_iota(jnp.int32, (n, n), 1)
    wide = jnp.broadcast_to(decay_row, (n, n))
    down = jnp.sum(jnp.where(col <= row, wide, 0.0), axis=1, keepdims=True)
    decay_col = jnp.sum(jnp.where(col == row, wide, 0.0), axis=1, keepdims=True)
    along = jnp.sum(jnp.where(row <= col, decay_col, 0.0), axis=0, keepdims=True)
    return down, along


def mark_kernel(done):
    done[...] = jnp.zeros_like(done)


def project_kernel(
    x0, x1, x2, x3, y0, y1, y2, y3, gain, decay, dk, dv, wk, wv, done, normed, packed, ret_k, ret_v
):
    rows, head = ret_k.shape
    chip = lax.axis_index("fs")
    core = lax.axis_index("tp")
    for j, side in enumerate(((x0, x1, x2, x3), (y0, y1, y2, y3))):
        for k, piece in enumerate(side):
            own = piece.shape[0]
            wide = piece[...].astype(F32)
            scale = lax.rsqrt(jnp.mean(wide * wide, axis=-1, keepdims=True) + EPS)
            at = pl.multiple_of(((chip ^ k) * 2 + (core ^ j)) * own, own)
            normed[pl.ds(at, own), :] = (wide * scale * gain[...]).astype(BF16)
    rounded = normed[...]
    packed[0:rows, :] = nt(rounded, dk[...].reshape(-1, dk.shape[2])).astype(BF16)
    packed[rows : 2 * rows, :] = nn(rounded, dv[...]).astype(BF16)
    k = nn(rounded, wk[...]).astype(BF16)
    v = nn(rounded, wv[...]).astype(BF16)
    ret_k[...] = k
    ret_v[...] = v
    cumul, _ = cumulated(decay[...])
    last = cumul[rows - 1 :, :]
    state = tn(k.astype(F32) * (jnp.exp(last - cumul) * head ** (-0.5)), v.astype(F32), precision=HIGHEST)
    packed[2 * rows : 2 * rows + head, :] = state.astype(BF16)
    packed[2 * rows + head :, :] = jnp.broadcast_to(jnp.exp(last), (8, head)).astype(BF16)


def own_kernel(
    lam, normed, packed, ret_k, ret_v, decay, wq, dq, ret_gain, diff_gain, start,
    queries, scaled, inner, sums, stats, small, init,
):
    rows, head = ret_k.shape
    small[0:8, :] = jnp.broadcast_to(ret_gain[...], (8, head))
    small[8:16, :] = jnp.broadcast_to(diff_gain[...], (8, head))
    small[16:24, :] = jnp.full((8, head), lam[0])
    init[...] = start[0].astype(F32)
    x = normed[...]
    cumul, along = cumulated(decay[...])
    lower = at_or_before(rows)
    q = nn(x, wq[...]).astype(BF16)
    weights = nt(q, ret_k[...]) * head ** (-0.5) * jnp.exp(jnp.where(lower, cumul - along, -HUGE))
    inner[...] = nn(weights.astype(BF16), ret_v[...])
    scaled[...] = q.astype(F32) * jnp.exp(cumul)
    both = nt(x, dq[...].reshape(-1, dq.shape[2])).astype(BF16)
    queries[...] = both
    half = head // 2
    keys = packed[0:rows, :]
    values = packed[rows : 2 * rows, :]
    for m in range(2):
        s = nt(both[:, m * half : (m + 1) * half], keys[:, m * half : (m + 1) * half]) * half ** (-0.5)
        s = jnp.where(lower, s, -HUGE)
        top = jnp.max(s, axis=-1, keepdims=True)
        e = jnp.exp(s - top)
        sums[m] = nn(e.astype(BF16), values)
        stats[m] = jnp.concatenate([jnp.broadcast_to(top, (rows, half)), jnp.broadcast_to(jnp.sum(e, axis=-1, keepdims=True), (rows, half))], axis=1)


def finish_kernel(sources, *refs):
    count = len(sources) + 1
    queries, scaled, inner, sums, stats, small, init = refs[:7]
    blocks = refs[7 : 6 + count]
    weights = refs[6 + count : 6 + 2 * count]
    *outs, mixed = refs[6 + 2 * count :]
    keeps, sends = outs[: len(outs) // 2], outs[len(outs) // 2 :]
    rows, head = inner.shape
    half = head // 2
    place = lax.axis_index("sp")
    core = lax.axis_index("tp")
    chip = lax.axis_index("fs")
    source = [f(place) for f in sources]
    before = [jnp.logical_and(at >= 0, at < place) for at in source]
    factors = [b[2 * rows + head : 2 * rows + head + 8, :].astype(F32)[0:1, :] for b in blocks]
    entering = init[...]
    for factor, here in zip(factors, before):
        entering = entering * jnp.where(here, factor, 1.0)
    for j, block in enumerate(blocks):
        carry = jnp.where(before[j], 1.0, 0.0) * jnp.ones((1, head), F32)
        for i, factor in enumerate(factors):
            if i != j:
                carry = carry * jnp.where(jnp.logical_and(source[i] > source[j], before[i]), factor, 1.0)
        entering = entering + carry * block[2 * rows : 2 * rows + head, :].astype(F32)
    ret_out = inner[...] + nn(scaled[...], entering, precision=HIGHEST)
    centre = ret_out - jnp.mean(ret_out, axis=-1, keepdims=True)
    spread = lax.rsqrt(jnp.mean(centre * centre, axis=-1, keepdims=True) + EPS)
    ret_mix = (centre * spread * small[0:1, :]).astype(BF16)

    keys = jnp.concatenate([b[0:rows, :] for b in blocks], axis=0)
    values = jnp.concatenate([b[rows : 2 * rows, :] for b in blocks], axis=0)
    allowed = jnp.concatenate([jnp.full((1, rows), jnp.where(here, 1, 0)) for here in before], axis=1) > 0
    maps = []
    for m in range(2):
        s = nt(queries[:, m * half : (m + 1) * half], keys[:, m * half : (m + 1) * half]) * half ** (-0.5)
        s = jnp.where(allowed, s, -HUGE)
        old_top = stats[m][:, 0:1]
        old_total = stats[m][:, half : half + 1]
        top = jnp.maximum(old_top, jnp.max(s, axis=-1, keepdims=True))
        e = jnp.exp(s - top)
        kept = jnp.exp(old_top - top)
        total = old_total * kept + jnp.sum(e, axis=-1, keepdims=True)
        maps.append((sums[m] * kept + nn(e.astype(BF16), values)) / total)
    diff_out = maps[0] - small[16:17, :] * maps[1]
    level = lax.rsqrt(jnp.mean(diff_out * diff_out, axis=-1, keepdims=True) + EPS)
    diff_mix = (diff_out * level * small[8:9, :]).astype(BF16)

    mixed[:, :, :, :head] = ret_mix.reshape(mixed.shape[:3] + (head,))
    mixed[:, :, :, head:] = diff_mix.reshape(mixed.shape[:3] + (head,))
    ordered = jnp.concatenate([mixed[chip ^ k, core ^ j] for j in range(2) for k in range(mixed.shape[0])], axis=0)
    for k, w in enumerate(weights):
        cols = w.shape[2]
        at = pl.ds(pl.multiple_of((place ^ k) * cols, cols), cols)
        result = nn(ordered, w[...].reshape(2 * head, cols))
        own = keeps[0].shape[0]
        for i, (keep, send) in enumerate(zip(keeps, sends)):
            keep[:, at] = result[i * own : (i + 1) * own]
            send[:, at] = result[rows // 2 + i * own : rows // 2 + (i + 1) * own].astype(BF16)


def call(kernel, outs, flops, here, away=0, scratch=(), scalars=0):
    spots = [pltpu.SMEM] * scalars + [pltpu.VMEM] * here + [pltpu.HBM] * away
    run = pl.pallas_call(
        kernel,
        out_shape=outs,
        in_specs=[pl.BlockSpec(memory_space=spot) for spot in spots],
        out_specs=[pl.BlockSpec(memory_space=pltpu.VMEM)] * len(outs),
        scratch_shapes=list(scratch) + ([pltpu.SemaphoreType.DMA((away,))] if away else []),
        compiler_params=pltpu.CompilerParams(vmem_limit_bytes=24 * 1024 * 1024),
        cost_estimate=pl.CostEstimate(flops=flops, bytes_accessed=1 << 20, transcendentals=1 << 16),
    )

    def placed(*args):
        return run(*[a if spot is pltpu.SMEM else pltpu.with_memory_space_constraint(a, spot) for a, spot in zip(args, spots)])

    return placed


def shape(dims, kind):
    return pltpu.VMEM(dims, kind)


def local_few(
    tokens, in_gain, ret_query, ret_key, ret_value, decay_log, init_state, ret_gain,
    diff_query, diff_key, diff_value, diff_lambda, diff_gain, out_weight,
):
    head = ret_query.shape[1]
    width = tokens.shape[1]
    count = lax.axis_size("sp")
    group = lax.axis_size(("fs", "tp"))
    own_rows = tokens.shape[0]
    rows = own_rows * group

    def swapped(array, k):
        return lax.ppermute(array, "sp", [(i, i ^ k) for i in range(count)])

    weights = [out_weight] * count
    weights[1] = swapped(out_weight, 1)
    if count == 4:
        weights[2] = swapped(out_weight, 2)
        weights[3] = swapped(weights[2], 1)
    square = shape((rows, head), BF16)
    chips = lax.axis_size("fs")

    def across(array, k):
        return lax.ppermute(array, "fs", [(i, i ^ k) for i in range(chips)])

    def paired(array):
        return lax.ppermute(array, "tp", [(0, 1), (1, 0)])

    (done,) = call(mark_kernel, [shape((8, head), F32)], GATHER_FLOPS, 0)()
    near_rows, far_rows = [tokens], []
    for k in range(1, chips):
        near_rows.append(across(tokens, k))
    for k in range(chips):
        far_rows.append(paired(near_rows[k]))
    normed, packed, ret_k, ret_v = call(
        project_kernel, [shape((rows, width), BF16), shape((2 * rows + head + 8, head), BF16), square, square],
        2 * rows * width * head * 4, 15,
    )(
        *near_rows, *far_rows, in_gain[None, :], decay_log, jnp.swapaxes(diff_key, 1, 2), diff_value,
        ret_key, ret_value, done,
    )
    blocks, sources = [], []
    for d in range(1, count):
        pairs, source = route(d, count)
        sources.append(source)
        blocks.append(lax.ppermute(packed, "sp", pairs))
    wide = shape((rows, head), F32)
    pair = shape((2, rows, head), F32)
    mine = call(
        own_kernel, [square, wide, wide, pair, pair, shape((24, head), F32), shape((head, head), F32)],
        2 * rows * width * head * 2, 10, scalars=1,
    )(
        diff_lambda, normed, packed, ret_k, ret_v, decay_log, ret_query, jnp.swapaxes(diff_query, 1, 2),
        ret_gain[None, :], diff_gain[None, :], init_state,
    )
    part = (own_rows, width)
    outs = call(
        functools.partial(finish_kernel, sources), [shape(part, F32)] * chips + [shape(part, BF16)] * chips,
        2 * rows * width * head * 2, 6 + 2 * count, scratch=[pltpu.VMEM((chips, 2, own_rows, 2 * head), BF16)],
    )(*mine, *blocks, *weights)
    sums = []
    for k in range(chips):
        other = paired(outs[chips + k])
        sums.append(outs[k] + other.astype(F32))
    total = sums[0]
    for k in range(1, chips):
        total = total + across(sums[k].astype(BF16), k).astype(F32)
    return total.astype(BF16)


def local_many(
    tokens, in_gain, ret_query, ret_key, ret_value, decay_log, init_state, ret_gain,
    diff_query, diff_key, diff_value, diff_lambda, diff_gain, out_weight,
):
    head = ret_query.shape[1]
    width = tokens.shape[1]
    count = lax.axis_size("sp")
    place = lax.axis_index("sp")
    group = lax.axis_size(("fs", "tp"))
    own_rows = tokens.shape[0]
    rows = own_rows * group

    full_weight = lax.all_gather(out_weight, "sp", axis=2, tiled=True).reshape(2 * head, width)
    wide = lax.all_gather(tokens, ("fs", "tp"), axis=0, tiled=True).astype(F32)
    normed = (wide * lax.rsqrt(jnp.mean(wide * wide, axis=-1, keepdims=True) + EPS) * in_gain).astype(BF16)
    ret_q, ret_k, ret_v, diff_v = (nn(normed, w).astype(BF16) for w in (ret_query, ret_key, ret_value, diff_value))
    queries = [nn(normed, diff_query[m]).astype(BF16) for m in range(2)]
    keys = [nn(normed, diff_key[m]).astype(BF16) for m in range(2)]
    lower = at_or_before(rows)
    cumul, along = cumulated(decay_log)
    last = cumul[-1:, :]
    weighted = ret_k.astype(F32) * (jnp.exp(last - cumul) * head ** (-0.5))
    state = tn(weighted, ret_v.astype(F32), precision=HIGHEST)
    factor = jnp.broadcast_to(jnp.exp(last), (8, head))
    packed = jnp.concatenate([jnp.concatenate(keys, axis=1), diff_v, state.astype(BF16), factor.astype(BF16)], axis=0)
    every = lax.all_gather(packed, "sp")
    all_keys = every[:, :rows].reshape(count * rows, -1)
    all_values = every[:, rows : 2 * rows].reshape(count * rows, -1)

    def step(b, carried):
        block = lax.dynamic_index_in_dim(every, b, 0, False).astype(F32)
        return block[2 * rows + head, 0] * carried + block[2 * rows : 2 * rows + head]

    entering = lax.fori_loop(0, place, step, init_state[0].astype(F32))
    scores = nt(ret_q, ret_k) * head ** (-0.5) * jnp.exp(jnp.where(lower, cumul - along, -HUGE))
    ret_out = nn(scores.astype(BF16), ret_v) + nn(ret_q.astype(F32) * jnp.exp(cumul), entering, precision=HIGHEST)
    centre = ret_out - jnp.mean(ret_out, axis=-1, keepdims=True)
    ret_mix = (centre * lax.rsqrt(jnp.mean(centre * centre, axis=-1, keepdims=True) + EPS) * ret_gain).astype(BF16)

    maps = []
    half = head // 2
    allowed = jnp.arange(count * rows)[None, :] <= (place * rows + jnp.arange(rows))[:, None]
    for m in range(2):
        s = nt(queries[m], all_keys[:, m * half : (m + 1) * half]) * half ** (-0.5)
        s = jnp.where(allowed, s, -HUGE)
        e = jnp.exp(s - s.max(axis=-1, keepdims=True))
        maps.append(nn(e.astype(BF16), all_values) / e.sum(axis=-1, keepdims=True))
    diff_out = maps[0] - diff_lambda[0] * maps[1]
    level = lax.rsqrt(jnp.mean(diff_out * diff_out, axis=-1, keepdims=True) + EPS)
    diff_mix = (diff_out * level * diff_gain).astype(BF16)

    mixed = jnp.concatenate([ret_mix, diff_mix], axis=1)
    partial = nn(mixed, full_weight).astype(BF16)
    shares = lax.all_to_all(partial, ("fs", "tp"), 0, 0, tiled=True)
    return shares.reshape(group, own_rows, width).astype(F32).sum(axis=0).astype(BF16)


def solution(mesh):
    count = mesh.shape["sp"]
    in_specs = (
        P(("sp", "fs", "tp"), None),
        P(),
        P(None, ("fs", "tp")),
        P(None, ("fs", "tp")),
        P(None, ("fs", "tp")),
        P(("fs", "tp"), "sp"),
        P(("fs", "tp"), None, None),
        P(("fs", "tp")),
        P(None, None, ("fs", "tp")),
        P(None, None, ("fs", "tp")),
        P(None, ("fs", "tp")),
        P(("fs", "tp")),
        P(("fs", "tp")),
        P(None, ("fs", "tp"), "sp"),
    )
    out_specs = P(("sp", "fs", "tp"), None)
    local = local_few if few(count) and mesh.shape["fs"] == 4 and mesh.shape["tp"] == 2 else local_many
    step = jax.shard_map(local, mesh=mesh, in_specs=in_specs, out_specs=out_specs, check_vma=False)
    if local is local_many or count != 4:
        return step
    return step
```

```python
import functools

import jax
import jax.numpy as jnp
from jax import lax
from jax.experimental import pallas as pl
from jax.experimental.pallas import tpu as pltpu
from jax.sharding import PartitionSpec as P


EPS = 1e-06
HUGE = 1e30
HIGHEST = lax.Precision.HIGHEST
F32 = jnp.float32
BF16 = jnp.bfloat16

GATHER_FLOPS = 3 * 10**10


def dot(a, b, dims, **kw):
    return lax.dot_general(a, b, (dims, ((), ())), preferred_element_type=F32, **kw)


def nn(a, b, **kw):
    return dot(a, b, ((1,), (0,)), **kw)


def nt(a, b, **kw):
    return dot(a, b, ((1,), (1,)), **kw)


def tn(a, b, **kw):
    return dot(a, b, ((0,), (0,)), **kw)


def route(d, count):
    return [(i, i + d) for i in range(count - d)], lambda at: at - d


ROUNDS = (lambda at: lax.rem(2 * at + 1, 5), lambda at: lax.rem(3 * at + 2, 5))
ROUND_PAIRS = (((1, 0), (3, 1), (0, 2), (2, 3)), ((2, 0), (0, 1), (3, 2), (1, 3)))


def few(count):
    return count == 4


def at_or_before(n):
    return lax.broadcasted_iota(jnp.int32, (n, n), 1) <= lax.broadcasted_iota(jnp.int32, (n, n), 0)


def cumulated(decay_row):
    n = decay_row.shape[1]
    row = lax.broadcasted_iota(jnp.int32, (n, n), 0)
    col = lax.broadcasted_iota(jnp.int32, (n, n), 1)
    wide = jnp.broadcast_to(decay_row, (n, n))
    down = jnp.sum(jnp.where(col <= row, wide, 0.0), axis=1, keepdims=True)
    decay_col = jnp.sum(jnp.where(col == row, wide, 0.0), axis=1, keepdims=True)
    along = jnp.sum(jnp.where(row <= col, decay_col, 0.0), axis=0, keepdims=True)
    return down, along


def fetch(pairs, sems):
    copies = [pltpu.make_async_copy(src, dst, sems.at[i]) for i, (src, dst) in enumerate(pairs)]
    for copy in copies:
        copy.start()
    return copies


def prepare_kernel(
    decay_h, in_gain_h, ret_gain_h, diff_gain_h, init_h,
    key_scale, query_scale, fade, factor, gain, small, init, decay, in_gain, ret_gain, diff_gain, start, sems,
):
    head = factor.shape[1]
    copies = fetch(
        [(decay_h, decay), (in_gain_h, in_gain), (ret_gain_h, ret_gain), (diff_gain_h, diff_gain), (init_h, start)], sems
    )
    for copy in copies:
        copy.wait()
    cumul, along = cumulated(decay[...])
    rows = cumul.shape[0]
    last = cumul[rows - 1 :, :]
    key_scale[...] = jnp.broadcast_to(jnp.exp(last - cumul) * head ** (-0.5), (rows, head))
    query_scale[...] = jnp.broadcast_to(jnp.exp(cumul), (rows, head))
    fade[...] = jnp.exp(jnp.where(at_or_before(rows), cumul - along, -HUGE)) * head ** (-0.5)
    factor[...] = jnp.broadcast_to(jnp.exp(last), (8, head))
    gain[...] = in_gain[...]
    small[0:8, :] = jnp.broadcast_to(ret_gain[...], (8, head))
    small[8:16, :] = jnp.broadcast_to(diff_gain[...], (8, head))
    init[...] = start[0].astype(F32)


def project_kernel(
    x0, x1, x2, x3, y0, y1, y2, y3, gain, key_scale, factor, dk, dv, wk, wv, normed, packed, ret_k, ret_v
):
    rows, head = ret_k.shape
    chip = lax.axis_index("fs")
    core = lax.axis_index("tp")
    for j, side in enumerate(((x0, x1, x2, x3), (y0, y1, y2, y3))):
        for k, piece in enumerate(side):
            own = piece.shape[0]
            wide = piece[...].astype(F32)
            scale = lax.rsqrt(jnp.mean(wide * wide, axis=-1, keepdims=True) + EPS)
            at = pl.multiple_of(((chip ^ k) * 2 + (core ^ j)) * own, own)
            normed[pl.ds(at, own), :] = (wide * scale * gain[...]).astype(BF16)
    rounded = normed[...]
    packed[0:rows, :] = nt(rounded, dk[...].reshape(-1, dk.shape[2])).astype(BF16)
    packed[rows : 2 * rows, :] = nn(rounded, dv[...]).astype(BF16)
    k = nn(rounded, wk[...]).astype(BF16)
    v = nn(rounded, wv[...]).astype(BF16)
    ret_k[...] = k
    ret_v[...] = v
    state = tn(k.astype(F32) * key_scale[...], v.astype(F32), precision=HIGHEST)
    packed[2 * rows : 2 * rows + head, :] = state.astype(BF16)
    packed[2 * rows + head :, :] = factor[...].astype(BF16)


def own_kernel(lam, normed, packed, ret_k, ret_v, query_scale, fade, wq, dq, queries, scaled, inner, sums, stats, second):
    rows, head = ret_k.shape
    second[...] = jnp.full(second.shape, lam[0])
    x = normed[...]
    q = nn(x, wq[...]).astype(BF16)
    weights = nt(q, ret_k[...]) * fade[...]
    inner[...] = nn(weights.astype(BF16), ret_v[...])
    scaled[...] = q.astype(F32) * query_scale[...]
    both = nt(x, dq[...].reshape(-1, dq.shape[2])).astype(BF16)
    queries[...] = both
    half = head // 2
    lower = at_or_before(rows)
    keys = packed[0:rows, :]
    values = packed[rows : 2 * rows, :]
    for m in range(2):
        s = nt(both[:, m * half : (m + 1) * half], keys[:, m * half : (m + 1) * half]) * half ** (-0.5)
        s = jnp.where(lower, s, -HUGE)
        top = jnp.max(s, axis=-1, keepdims=True)
        e = jnp.exp(s - top)
        sums[m] = nn(e.astype(BF16), values)
        stats[m] = jnp.concatenate([jnp.broadcast_to(top, (rows, half)), jnp.broadcast_to(jnp.sum(e, axis=-1, keepdims=True), (rows, half))], axis=1)


def finish_kernel(sources, *refs):
    count = len(sources) + 1
    queries, scaled, inner, sums, stats, second, small, init = refs[:8]
    blocks = refs[8 : 7 + count]
    weights = refs[7 + count : -4]
    keep, send, order, mixed = refs[-4:]
    rows, head = inner.shape
    half = head // 2
    place = lax.axis_index("sp")
    core = lax.axis_index("tp")
    chip = lax.axis_index("fs")
    source = [f(place) for f in sources]
    before = [jnp.logical_and(at >= 0, at < place) for at in source]
    factors = [b[2 * rows + head : 2 * rows + head + 8, :].astype(F32)[0:1, :] for b in blocks]
    entering = init[...]
    for factor, here in zip(factors, before):
        entering = entering * jnp.where(here, factor, 1.0)
    for j, block in enumerate(blocks):
        carry = jnp.where(before[j], 1.0, 0.0) * jnp.ones((1, head), F32)
        for i, factor in enumerate(factors):
            if i != j:
                carry = carry * jnp.where(jnp.logical_and(source[i] > source[j], before[i]), factor, 1.0)
        entering = entering + carry * block[2 * rows : 2 * rows + head, :].astype(F32)
    ret_out = inner[...] + nn(scaled[...], entering, precision=HIGHEST)
    centre = ret_out - jnp.mean(ret_out, axis=-1, keepdims=True)
    spread = lax.rsqrt(jnp.mean(centre * centre, axis=-1, keepdims=True) + EPS)
    ret_mix = (centre * spread * small[0:1, :]).astype(BF16)

    keys = jnp.concatenate([b[0:rows, :] for b in blocks], axis=0)
    values = jnp.concatenate([b[rows : 2 * rows, :] for b in blocks], axis=0)
    allowed = jnp.concatenate([jnp.full((1, rows), jnp.where(here, 1, 0)) for here in before], axis=1) > 0
    maps = []
    for m in range(2):
        s = nt(queries[:, m * half : (m + 1) * half], keys[:, m * half : (m + 1) * half]) * half ** (-0.5)
        s = jnp.where(allowed, s, -HUGE)
        old_top = stats[m][:, 0:1]
        old_total = stats[m][:, half : half + 1]
        top = jnp.maximum(old_top, jnp.max(s, axis=-1, keepdims=True))
        e = jnp.exp(s - top)
        kept = jnp.exp(old_top - top)
        total = old_total * kept + jnp.sum(e, axis=-1, keepdims=True)
        maps.append((sums[m] * kept + nn(e.astype(BF16), values)) / total)
    diff_out = maps[0] - second[0:1, :] * maps[1]
    level = lax.rsqrt(jnp.mean(diff_out * diff_out, axis=-1, keepdims=True) + EPS)
    diff_mix = (diff_out * level * small[8:9, :]).astype(BF16)

    mixed[:, :, :, :head] = ret_mix.reshape(mixed.shape[:3] + (head,))
    mixed[:, :, :, head:] = diff_mix.reshape(mixed.shape[:3] + (head,))
    ordered = jnp.concatenate([mixed[chip ^ k, core ^ j] for j in range(2) for k in range(mixed.shape[0])], axis=0)
    order[...] = ordered
    cols = weights[0].shape[2]
    for k, w in enumerate(weights):
        result = nn(ordered, w[...].reshape(2 * head, cols))
        keep[:, k * cols : (k + 1) * cols] = result[: rows // 2]
        send[:, k * cols : (k + 1) * cols] = result[rows // 2 :].astype(BF16)


def pick_kernel(own, second, picked):
    picked[...] = jnp.where(lax.axis_index("sp") == 2, own[...], second[...])


def last_kernel(outer, inner, order, keep, send):
    kept = keep.shape[0]
    place = lax.axis_index("sp")
    weight = jnp.where(jnp.logical_or(place == 1, place == 2), inner[...], outer[...])
    result = nn(order[...], weight.reshape(-1, weight.shape[2]))
    keep[...] = result[:kept]
    send[...] = result[kept:].astype(BF16)


def merge_kernel(keep, other, last_keep, last_other, mine, *sends):
    own, _ = mine.shape
    cut = keep.shape[1]
    for k, target in enumerate((mine, *sends)):
        span = slice(k * own, (k + 1) * own)
        target[:, :cut] = (keep[span, :] + other[span, :].astype(F32)).astype(target.dtype)
        target[:, cut:] = (last_keep[span, :] + last_other[span, :].astype(F32)).astype(target.dtype)


def total_kernel(mine, *refs):
    *shares, out = refs
    total = mine[...]
    for share in shares:
        total = total + share[...].astype(F32)
    place = lax.axis_index("sp")
    cols = total.shape[1] // lax.axis_size("sp")
    for k, to in enumerate((place, ROUNDS[0](place), ROUNDS[1](place), place ^ 3)):
        at = pl.multiple_of(to * cols, cols)
        out[:, pl.ds(at, cols)] = total[:, k * cols : (k + 1) * cols].astype(BF16)


def call(kernel, outs, flops, here, away=0, scratch=(), scalars=0):
    spots = [pltpu.SMEM] * scalars + [pltpu.VMEM] * here + [pltpu.HBM] * away
    run = pl.pallas_call(
        kernel,
        out_shape=outs,
        in_specs=[pl.BlockSpec(memory_space=spot) for spot in spots],
        out_specs=[pl.BlockSpec(memory_space=pltpu.VMEM)] * len(outs),
        scratch_shapes=list(scratch) + ([pltpu.SemaphoreType.DMA((away,))] if away else []),
        compiler_params=pltpu.CompilerParams(vmem_limit_bytes=24 * 1024 * 1024),
        cost_estimate=pl.CostEstimate(flops=flops, bytes_accessed=1 << 20, transcendentals=1 << 16),
    )

    def placed(*args):
        return run(*[a if spot is pltpu.SMEM else pltpu.with_memory_space_constraint(a, spot) for a, spot in zip(args, spots)])

    return placed


def shape(dims, kind):
    return pltpu.VMEM(dims, kind)


def local_few(
    tokens, in_gain, ret_query, ret_key, ret_value, decay_log, init_state, ret_gain,
    diff_query, diff_key, diff_value, diff_lambda, diff_gain, out_weight,
):
    head = ret_query.shape[1]
    width = tokens.shape[1]
    count = lax.axis_size("sp")
    group = lax.axis_size(("fs", "tp"))
    own_rows = tokens.shape[0]
    rows = own_rows * group

    weights = [out_weight]
    for pairs in ROUND_PAIRS:
        weights.append(lax.ppermute(out_weight, "sp", list(pairs)))
    outer = lax.ppermute(weights[1], "sp", [(1, 0), (2, 3)])
    (picked,) = call(pick_kernel, [shape(out_weight.shape, BF16)], 1 << 17, 2)(out_weight, weights[2])
    inner = lax.ppermute(picked, "sp", [(2, 1), (3, 2)])
    square = shape((rows, head), BF16)
    chips = lax.axis_size("fs")
    line = pltpu.VMEM((1, head), F32)

    def across(array, k):
        return lax.ppermute(array, "fs", [(i, i ^ k) for i in range(chips)])

    def paired(array):
        return lax.ppermute(array, "tp", [(0, 1), (1, 0)])

    wide = shape((rows, head), F32)
    key_scale, query_scale, fade, factor, gain, small, init = call(
        prepare_kernel,
        [wide, wide, shape((rows, rows), F32), shape((8, head), F32), shape((1, width), F32),
         shape((16, head), F32), shape((head, head), F32)],
        GATHER_FLOPS, 0, 5, [line, pltpu.VMEM((1, width), F32), line, line, pltpu.VMEM((1, head, head), BF16)],
    )(decay_log, in_gain[None, :], ret_gain[None, :], diff_gain[None, :], init_state)
    near_rows, far_rows = [tokens], []
    for k in range(1, chips):
        near_rows.append(across(tokens, k))
    for k in range(chips):
        far_rows.append(paired(near_rows[k]))
    normed, packed, ret_k, ret_v = call(
        project_kernel, [shape((rows, width), BF16), shape((2 * rows + head + 8, head), BF16), square, square],
        2 * rows * width * head * 4, 15,
    )(*near_rows, *far_rows, gain, key_scale, factor, jnp.swapaxes(diff_key, 1, 2), diff_value, ret_key, ret_value)
    blocks, sources = [], []
    for d in range(1, count):
        pairs, source = route(d, count)
        sources.append(source)
        blocks.append(lax.ppermute(packed, "sp", pairs))
    pair = shape((2, rows, head), F32)
    mine = call(
        own_kernel, [square, wide, wide, pair, pair, shape((8, head), F32)], 2 * rows * width * head * 2, 8, scalars=1,
    )(diff_lambda, normed, packed, ret_k, ret_v, query_scale, fade, ret_query, jnp.swapaxes(diff_query, 1, 2))
    cols = out_weight.shape[2]
    half, most = rows // 2, (count - 1) * cols
    keep, send, order = call(
        functools.partial(finish_kernel, sources),
        [shape((half, most), F32), shape((half, most), BF16), shape((rows, 2 * head), BF16)],
        2 * rows * width * head * 2, 6 + 2 * count, scratch=[pltpu.VMEM((chips, 2, own_rows, 2 * head), BF16)],
    )(*mine, small, init, *blocks, *weights)
    other = paired(send)
    last_keep, last_send = call(
        last_kernel, [shape((half, cols), F32), shape((half, cols), BF16)], 2 * rows * cols * head * 2, 3
    )(outer, inner, order)
    last_other = paired(last_send)
    part = (own_rows, width)
    kept, *shares = call(merge_kernel, [shape(part, F32)] + [shape(part, BF16)] * (chips - 1), 1 << 18, 4)(
        keep, other, last_keep, last_other
    )
    arrived = []
    for k in range(1, chips):
        arrived.append(across(shares[k - 1], k))
    (out,) = call(total_kernel, [jax.ShapeDtypeStruct(part, BF16)], 1 << 18, chips)(kept, *arrived)
    return out


def local_many(
    tokens, in_gain, ret_query, ret_key, ret_value, decay_log, init_state, ret_gain,
    diff_query, diff_key, diff_value, diff_lambda, diff_gain, out_weight,
):
    head = ret_query.shape[1]
    width = tokens.shape[1]
    count = lax.axis_size("sp")
    place = lax.axis_index("sp")
    group = lax.axis_size(("fs", "tp"))
    own_rows = tokens.shape[0]
    rows = own_rows * group

    full_weight = lax.all_gather(out_weight, "sp", axis=2, tiled=True).reshape(2 * head, width)
    wide = lax.all_gather(tokens, ("fs", "tp"), axis=0, tiled=True).astype(F32)
    normed = (wide * lax.rsqrt(jnp.mean(wide * wide, axis=-1, keepdims=True) + EPS) * in_gain).astype(BF16)
    ret_q, ret_k, ret_v, diff_v = (nn(normed, w).astype(BF16) for w in (ret_query, ret_key, ret_value, diff_value))
    queries = [nn(normed, diff_query[m]).astype(BF16) for m in range(2)]
    keys = [nn(normed, diff_key[m]).astype(BF16) for m in range(2)]
    lower = at_or_before(rows)
    cumul, along = cumulated(decay_log)
    last = cumul[-1:, :]
    weighted = ret_k.astype(F32) * (jnp.exp(last - cumul) * head ** (-0.5))
    state = tn(weighted, ret_v.astype(F32), precision=HIGHEST)
    factor = jnp.broadcast_to(jnp.exp(last), (8, head))
    packed = jnp.concatenate([jnp.concatenate(keys, axis=1), diff_v, state.astype(BF16), factor.astype(BF16)], axis=0)
    every = lax.all_gather(packed, "sp")
    all_keys = every[:, :rows].reshape(count * rows, -1)
    all_values = every[:, rows : 2 * rows].reshape(count * rows, -1)

    def step(b, carried):
        block = lax.dynamic_index_in_dim(every, b, 0, False).astype(F32)
        return block[2 * rows + head, 0] * carried + block[2 * rows : 2 * rows + head]

    entering = lax.fori_loop(0, place, step, init_state[0].astype(F32))
    scores = nt(ret_q, ret_k) * head ** (-0.5) * jnp.exp(jnp.where(lower, cumul - along, -HUGE))
    ret_out = nn(scores.astype(BF16), ret_v) + nn(ret_q.astype(F32) * jnp.exp(cumul), entering, precision=HIGHEST)
    centre = ret_out - jnp.mean(ret_out, axis=-1, keepdims=True)
    ret_mix = (centre * lax.rsqrt(jnp.mean(centre * centre, axis=-1, keepdims=True) + EPS) * ret_gain).astype(BF16)

    maps = []
    half = head // 2
    allowed = jnp.arange(count * rows)[None, :] <= (place * rows + jnp.arange(rows))[:, None]
    for m in range(2):
        s = nt(queries[m], all_keys[:, m * half : (m + 1) * half]) * half ** (-0.5)
        s = jnp.where(allowed, s, -HUGE)
        e = jnp.exp(s - s.max(axis=-1, keepdims=True))
        maps.append(nn(e.astype(BF16), all_values) / e.sum(axis=-1, keepdims=True))
    diff_out = maps[0] - diff_lambda[0] * maps[1]
    level = lax.rsqrt(jnp.mean(diff_out * diff_out, axis=-1, keepdims=True) + EPS)
    diff_mix = (diff_out * level * diff_gain).astype(BF16)

    mixed = jnp.concatenate([ret_mix, diff_mix], axis=1)
    partial = nn(mixed, full_weight).astype(BF16)
    shares = lax.all_to_all(partial, ("fs", "tp"), 0, 0, tiled=True)
    return shares.reshape(group, own_rows, width).astype(F32).sum(axis=0).astype(BF16)


def solution(mesh):
    count = mesh.shape["sp"]
    in_specs = (
        P(("sp", "fs", "tp"), None),
        P(),
        P(None, ("fs", "tp")),
        P(None, ("fs", "tp")),
        P(None, ("fs", "tp")),
        P(("fs", "tp"), "sp"),
        P(("fs", "tp"), None, None),
        P(("fs", "tp")),
        P(None, None, ("fs", "tp")),
        P(None, None, ("fs", "tp")),
        P(None, ("fs", "tp")),
        P(("fs", "tp")),
        P(("fs", "tp")),
        P(None, ("fs", "tp"), "sp"),
    )
    out_specs = P(("sp", "fs", "tp"), None)
    local = local_few if few(count) and mesh.shape["fs"] == 4 and mesh.shape["tp"] == 2 else local_many
    step = jax.shard_map(local, mesh=mesh, in_specs=in_specs, out_specs=out_specs, check_vma=False)
    if local is local_many:
        return step
    return step
```

```python
import functools

import jax
import jax.numpy as jnp
from jax import lax
from jax.experimental import pallas as pl
from jax.experimental.pallas import tpu as pltpu
from jax.sharding import PartitionSpec as P


EPS = 1e-06
HUGE = 1e30
HIGHEST = lax.Precision.HIGHEST
F32 = jnp.float32
BF16 = jnp.bfloat16

GATHER_FLOPS = 3 * 10**10


def dot(a, b, dims, **kw):
    return lax.dot_general(a, b, (dims, ((), ())), preferred_element_type=F32, **kw)


def nn(a, b, **kw):
    return dot(a, b, ((1,), (0,)), **kw)


def nt(a, b, **kw):
    return dot(a, b, ((1,), (1,)), **kw)


def tn(a, b, **kw):
    return dot(a, b, ((0,), (0,)), **kw)


def route(d, count):
    return [(i, i + d) for i in range(count - d)], lambda at: at - d


ROUNDS = (lambda at: lax.rem(2 * at + 1, 5), lambda at: lax.rem(3 * at + 2, 5))
ROUND_PAIRS = (((1, 0), (3, 1), (0, 2), (2, 3)), ((2, 0), (0, 1), (3, 2), (1, 3)))


def halves(a):
    high = a.astype(BF16)
    return high, (a - high.astype(F32)).astype(BF16)


def few(count):
    return count == 4


def at_or_before(n):
    return lax.broadcasted_iota(jnp.int32, (n, n), 1) <= lax.broadcasted_iota(jnp.int32, (n, n), 0)


def cumulated(decay_row):
    n = decay_row.shape[1]
    row = lax.broadcasted_iota(jnp.int32, (n, n), 0)
    col = lax.broadcasted_iota(jnp.int32, (n, n), 1)
    wide = jnp.broadcast_to(decay_row, (n, n))
    down = jnp.sum(jnp.where(col <= row, wide, 0.0), axis=1, keepdims=True)
    decay_col = jnp.sum(jnp.where(col == row, wide, 0.0), axis=1, keepdims=True)
    along = jnp.sum(jnp.where(row <= col, decay_col, 0.0), axis=0, keepdims=True)
    return down, along


def fetch(pairs, sems):
    copies = [pltpu.make_async_copy(src, dst, sems.at[i]) for i, (src, dst) in enumerate(pairs)]
    for copy in copies:
        copy.start()
    return copies


def prepare_kernel(
    decay_h, in_gain_h, ret_gain_h, diff_gain_h, init_h,
    key_scale, query_scale, fade, factor, gain, small, init, decay, in_gain, ret_gain, diff_gain, start, sems,
):
    head = factor.shape[1]
    copies = fetch(
        [(decay_h, decay), (in_gain_h, in_gain), (ret_gain_h, ret_gain), (diff_gain_h, diff_gain), (init_h, start)], sems
    )
    for copy in copies:
        copy.wait()
    cumul, along = cumulated(decay[...])
    rows = cumul.shape[0]
    last = cumul[rows - 1 :, :]
    key_scale[...] = jnp.broadcast_to(jnp.exp(last - cumul) * head ** (-0.5), (rows, head))
    query_scale[...] = jnp.broadcast_to(jnp.exp(cumul), (rows, head))
    fade[...] = jnp.exp(jnp.where(at_or_before(rows), cumul - along, -HUGE)) * head ** (-0.5)
    factor[...] = jnp.broadcast_to(jnp.exp(last), (8, head))
    gain[...] = in_gain[...]
    small[0:8, :] = jnp.broadcast_to(ret_gain[...], (8, head))
    small[8:16, :] = jnp.broadcast_to(diff_gain[...], (8, head))
    init[...] = start[0].astype(F32)


def project_kernel(
    x0, x1, x2, x3, y0, y1, y2, y3, gain, key_scale, factor, dk, dv, wk, wv, normed, packed, ret_k, ret_v
):
    rows, head = ret_k.shape
    chip = lax.axis_index("fs")
    core = lax.axis_index("tp")
    for j, side in enumerate(((x0, x1, x2, x3), (y0, y1, y2, y3))):
        for k, piece in enumerate(side):
            own = piece.shape[0]
            wide = piece[...].astype(F32)
            scale = lax.rsqrt(jnp.mean(wide * wide, axis=-1, keepdims=True) + EPS)
            at = pl.multiple_of(((chip ^ k) * 2 + (core ^ j)) * own, own)
            normed[pl.ds(at, own), :] = (wide * scale * gain[...]).astype(BF16)
    rounded = normed[...]
    packed[0:rows, :] = nt(rounded, dk[...].reshape(-1, dk.shape[2])).astype(BF16)
    packed[rows : 2 * rows, :] = nn(rounded, dv[...]).astype(BF16)
    k = nn(rounded, wk[...]).astype(BF16)
    v = nn(rounded, wv[...]).astype(BF16)
    ret_k[...] = k
    ret_v[...] = v
    weighted, rest = halves(k.astype(F32) * key_scale[...])
    state = tn(weighted, v) + tn(rest, v)
    packed[2 * rows : 2 * rows + head, :] = state.astype(BF16)
    packed[2 * rows + head :, :] = factor[...].astype(BF16)


def own_kernel(lam, normed, packed, ret_k, ret_v, query_scale, fade, wq, dq, queries, scaled, inner, sums, stats, second):
    rows, head = ret_k.shape
    second[...] = jnp.full(second.shape, lam[0])
    x = normed[...]
    q = nn(x, wq[...]).astype(BF16)
    weights = nt(q, ret_k[...]) * fade[...]
    inner[...] = nn(weights.astype(BF16), ret_v[...])
    scaled[...] = q.astype(F32) * query_scale[...]
    both = nt(x, dq[...].reshape(-1, dq.shape[2])).astype(BF16)
    queries[...] = both
    half = head // 2
    lower = at_or_before(rows)
    keys = packed[0:rows, :]
    values = packed[rows : 2 * rows, :]
    for m in range(2):
        s = nt(both[:, m * half : (m + 1) * half], keys[:, m * half : (m + 1) * half]) * half ** (-0.5)
        s = jnp.where(lower, s, -HUGE)
        top = jnp.max(s, axis=-1, keepdims=True)
        e = jnp.exp(s - top)
        sums[m] = nn(e.astype(BF16), values)
        stats[m] = jnp.concatenate([jnp.broadcast_to(top, (rows, half)), jnp.broadcast_to(jnp.sum(e, axis=-1, keepdims=True), (rows, half))], axis=1)


def finish_kernel(sources, *refs):
    count = len(sources) + 1
    queries, scaled, inner, sums, stats, second, small, init = refs[:8]
    blocks = refs[8 : 7 + count]
    weights = refs[7 + count : -4]
    keep, send, order, mixed = refs[-4:]
    rows, head = inner.shape
    half = head // 2
    place = lax.axis_index("sp")
    core = lax.axis_index("tp")
    chip = lax.axis_index("fs")
    source = [f(place) for f in sources]
    before = [jnp.logical_and(at >= 0, at < place) for at in source]
    factors = [b[2 * rows + head : 2 * rows + head + 8, :].astype(F32)[0:1, :] for b in blocks]
    entering = init[...]
    for factor, here in zip(factors, before):
        entering = entering * jnp.where(here, factor, 1.0)
    for j, block in enumerate(blocks):
        carry = jnp.where(before[j], 1.0, 0.0) * jnp.ones((1, head), F32)
        for i, factor in enumerate(factors):
            if i != j:
                carry = carry * jnp.where(jnp.logical_and(source[i] > source[j], before[i]), factor, 1.0)
        entering = entering + carry * block[2 * rows : 2 * rows + head, :].astype(F32)
    (left, left_rest), (right, right_rest) = halves(scaled[...]), halves(entering)
    ret_out = inner[...] + nn(left, right) + nn(left, right_rest) + nn(left_rest, right)
    centre = ret_out - jnp.mean(ret_out, axis=-1, keepdims=True)
    spread = lax.rsqrt(jnp.mean(centre * centre, axis=-1, keepdims=True) + EPS)
    ret_mix = (centre * spread * small[0:1, :]).astype(BF16)

    keys = jnp.concatenate([b[0:rows, :] for b in blocks], axis=0)
    values = jnp.concatenate([b[rows : 2 * rows, :] for b in blocks], axis=0)
    allowed = jnp.concatenate([jnp.full((1, rows), jnp.where(here, 1, 0)) for here in before], axis=1) > 0
    maps = []
    for m in range(2):
        s = nt(queries[:, m * half : (m + 1) * half], keys[:, m * half : (m + 1) * half]) * half ** (-0.5)
        s = jnp.where(allowed, s, -HUGE)
        old_top = stats[m][:, 0:1]
        old_total = stats[m][:, half : half + 1]
        top = jnp.maximum(old_top, jnp.max(s, axis=-1, keepdims=True))
        e = jnp.exp(s - top)
        kept = jnp.exp(old_top - top)
        total = old_total * kept + jnp.sum(e, axis=-1, keepdims=True)
        maps.append((sums[m] * kept + nn(e.astype(BF16), values)) / total)
    diff_out = maps[0] - second[0:1, :] * maps[1]
    level = lax.rsqrt(jnp.mean(diff_out * diff_out, axis=-1, keepdims=True) + EPS)
    diff_mix = (diff_out * level * small[8:9, :]).astype(BF16)

    mixed[:, :, :, :head] = ret_mix.reshape(mixed.shape[:3] + (head,))
    mixed[:, :, :, head:] = diff_mix.reshape(mixed.shape[:3] + (head,))
    ordered = jnp.concatenate([mixed[chip ^ k, core ^ j] for j in range(2) for k in range(mixed.shape[0])], axis=0)
    order[...] = ordered
    cols = weights[0].shape[2]
    for k, w in enumerate(weights):
        result = nn(ordered, w[...].reshape(2 * head, cols))
        keep[:, k * cols : (k + 1) * cols] = result[: rows // 2]
        send[:, k * cols : (k + 1) * cols] = result[rows // 2 :].astype(BF16)


def pick_kernel(own, second, picked):
    picked[...] = jnp.where(lax.axis_index("sp") == 2, own[...], second[...])


def last_kernel(outer, inner, order, keep, send):
    kept = keep.shape[0]
    place = lax.axis_index("sp")
    weight = jnp.where(jnp.logical_or(place == 1, place == 2), inner[...], outer[...])
    result = nn(order[...], weight.reshape(-1, weight.shape[2]))
    keep[...] = result[:kept]
    send[...] = result[kept:].astype(BF16)


def merge_kernel(keep, other, last_keep, last_other, mine, *sends):
    own, _ = mine.shape
    cut = keep.shape[1]
    for k, target in enumerate((mine, *sends)):
        span = slice(k * own, (k + 1) * own)
        target[:, :cut] = (keep[span, :] + other[span, :].astype(F32)).astype(target.dtype)
        target[:, cut:] = (last_keep[span, :] + last_other[span, :].astype(F32)).astype(target.dtype)


def total_kernel(mine, *refs):
    *shares, out = refs
    total = mine[...]
    for share in shares:
        total = total + share[...].astype(F32)
    place = lax.axis_index("sp")
    cols = total.shape[1] // lax.axis_size("sp")
    for k, to in enumerate((place, ROUNDS[0](place), ROUNDS[1](place), place ^ 3)):
        at = pl.multiple_of(to * cols, cols)
        out[:, pl.ds(at, cols)] = total[:, k * cols : (k + 1) * cols].astype(BF16)


def call(kernel, outs, flops, here, away=0, scratch=(), scalars=0):
    spots = [pltpu.SMEM] * scalars + [pltpu.VMEM] * here + [pltpu.HBM] * away
    run = pl.pallas_call(
        kernel,
        out_shape=outs,
        in_specs=[pl.BlockSpec(memory_space=spot) for spot in spots],
        out_specs=[pl.BlockSpec(memory_space=pltpu.VMEM)] * len(outs),
        scratch_shapes=list(scratch) + ([pltpu.SemaphoreType.DMA((away,))] if away else []),
        compiler_params=pltpu.CompilerParams(vmem_limit_bytes=24 * 1024 * 1024),
        cost_estimate=pl.CostEstimate(flops=flops, bytes_accessed=1 << 20, transcendentals=1 << 16),
    )

    def placed(*args):
        return run(*[a if spot is pltpu.SMEM else pltpu.with_memory_space_constraint(a, spot) for a, spot in zip(args, spots)])

    return placed


def shape(dims, kind):
    return pltpu.VMEM(dims, kind)


def local_few(
    tokens, in_gain, ret_query, ret_key, ret_value, decay_log, init_state, ret_gain,
    diff_query, diff_key, diff_value, diff_lambda, diff_gain, out_weight,
):
    head = ret_query.shape[1]
    width = tokens.shape[1]
    count = lax.axis_size("sp")
    group = lax.axis_size(("fs", "tp"))
    own_rows = tokens.shape[0]
    rows = own_rows * group

    weights = [out_weight]
    for pairs in ROUND_PAIRS:
        weights.append(lax.ppermute(out_weight, "sp", list(pairs)))
    outer = lax.ppermute(weights[1], "sp", [(1, 0), (2, 3)])
    (picked,) = call(pick_kernel, [shape(out_weight.shape, BF16)], 1 << 17, 2)(out_weight, weights[2])
    inner = lax.ppermute(picked, "sp", [(2, 1), (3, 2)])
    square = shape((rows, head), BF16)
    chips = lax.axis_size("fs")
    line = pltpu.VMEM((1, head), F32)

    def across(array, k):
        return lax.ppermute(array, "fs", [(i, i ^ k) for i in range(chips)])

    def paired(array):
        return lax.ppermute(array, "tp", [(0, 1), (1, 0)])

    wide = shape((rows, head), F32)
    key_scale, query_scale, fade, factor, gain, small, init = call(
        prepare_kernel,
        [wide, wide, shape((rows, rows), F32), shape((8, head), F32), shape((1, width), F32),
         shape((16, head), F32), shape((head, head), F32)],
        GATHER_FLOPS, 0, 5, [line, pltpu.VMEM((1, width), F32), line, line, pltpu.VMEM((1, head, head), BF16)],
    )(decay_log, in_gain[None, :], ret_gain[None, :], diff_gain[None, :], init_state)
    near_rows, far_rows = [tokens], []
    for k in range(1, chips):
        near_rows.append(across(tokens, k))
    for k in range(chips):
        far_rows.append(paired(near_rows[k]))
    normed, packed, ret_k, ret_v = call(
        project_kernel, [shape((rows, width), BF16), shape((2 * rows + head + 8, head), BF16), square, square],
        2 * rows * width * head * 4, 15,
    )(*near_rows, *far_rows, gain, key_scale, factor, jnp.swapaxes(diff_key, 1, 2), diff_value, ret_key, ret_value)
    blocks, sources = [], []
    for d in range(1, count):
        pairs, source = route(d, count)
        sources.append(source)
        blocks.append(lax.ppermute(packed, "sp", pairs))
    pair = shape((2, rows, head), F32)
    mine = call(
        own_kernel, [square, wide, wide, pair, pair, shape((8, head), F32)], 2 * rows * width * head * 2, 8, scalars=1,
    )(diff_lambda, normed, packed, ret_k, ret_v, query_scale, fade, ret_query, jnp.swapaxes(diff_query, 1, 2))
    cols = out_weight.shape[2]
    half, most = rows // 2, (count - 1) * cols
    keep, send, order = call(
        functools.partial(finish_kernel, sources),
        [shape((half, most), F32), shape((half, most), BF16), shape((rows, 2 * head), BF16)],
        2 * rows * width * head * 2, 6 + 2 * count, scratch=[pltpu.VMEM((chips, 2, own_rows, 2 * head), BF16)],
    )(*mine, small, init, *blocks, *weights)
    other = paired(send)
    last_keep, last_send = call(
        last_kernel, [shape((half, cols), F32), shape((half, cols), BF16)], 2 * rows * cols * head * 2, 3
    )(outer, inner, order)
    last_other = paired(last_send)
    part = (own_rows, width)
    kept, *shares = call(merge_kernel, [shape(part, F32)] + [shape(part, BF16)] * (chips - 1), 1 << 18, 4)(
        keep, other, last_keep, last_other
    )
    arrived = []
    for k in range(1, chips):
        arrived.append(across(shares[k - 1], k))
    (out,) = call(total_kernel, [jax.ShapeDtypeStruct(part, BF16)], 1 << 18, chips)(kept, *arrived)
    return out


def local_many(
    tokens, in_gain, ret_query, ret_key, ret_value, decay_log, init_state, ret_gain,
    diff_query, diff_key, diff_value, diff_lambda, diff_gain, out_weight,
):
    head = ret_query.shape[1]
    width = tokens.shape[1]
    count = lax.axis_size("sp")
    place = lax.axis_index("sp")
    group = lax.axis_size(("fs", "tp"))
    own_rows = tokens.shape[0]
    rows = own_rows * group

    full_weight = lax.all_gather(out_weight, "sp", axis=2, tiled=True).reshape(2 * head, width)
    wide = lax.all_gather(tokens, ("fs", "tp"), axis=0, tiled=True).astype(F32)
    normed = (wide * lax.rsqrt(jnp.mean(wide * wide, axis=-1, keepdims=True) + EPS) * in_gain).astype(BF16)
    ret_q, ret_k, ret_v, diff_v = (nn(normed, w).astype(BF16) for w in (ret_query, ret_key, ret_value, diff_value))
    queries = [nn(normed, diff_query[m]).astype(BF16) for m in range(2)]
    keys = [nn(normed, diff_key[m]).astype(BF16) for m in range(2)]
    lower = at_or_before(rows)
    cumul, along = cumulated(decay_log)
    last = cumul[-1:, :]
    weighted = ret_k.astype(F32) * (jnp.exp(last - cumul) * head ** (-0.5))
    state = tn(weighted, ret_v.astype(F32), precision=HIGHEST)
    factor = jnp.broadcast_to(jnp.exp(last), (8, head))
    packed = jnp.concatenate([jnp.concatenate(keys, axis=1), diff_v, state.astype(BF16), factor.astype(BF16)], axis=0)
    every = lax.all_gather(packed, "sp")
    all_keys = every[:, :rows].reshape(count * rows, -1)
    all_values = every[:, rows : 2 * rows].reshape(count * rows, -1)

    def step(b, carried):
        block = lax.dynamic_index_in_dim(every, b, 0, False).astype(F32)
        return block[2 * rows + head, 0] * carried + block[2 * rows : 2 * rows + head]

    entering = lax.fori_loop(0, place, step, init_state[0].astype(F32))
    scores = nt(ret_q, ret_k) * head ** (-0.5) * jnp.exp(jnp.where(lower, cumul - along, -HUGE))
    ret_out = nn(scores.astype(BF16), ret_v) + nn(ret_q.astype(F32) * jnp.exp(cumul), entering, precision=HIGHEST)
    centre = ret_out - jnp.mean(ret_out, axis=-1, keepdims=True)
    ret_mix = (centre * lax.rsqrt(jnp.mean(centre * centre, axis=-1, keepdims=True) + EPS) * ret_gain).astype(BF16)

    maps = []
    half = head // 2
    allowed = jnp.arange(count * rows)[None, :] <= (place * rows + jnp.arange(rows))[:, None]
    for m in range(2):
        s = nt(queries[m], all_keys[:, m * half : (m + 1) * half]) * half ** (-0.5)
        s = jnp.where(allowed, s, -HUGE)
        e = jnp.exp(s - s.max(axis=-1, keepdims=True))
        maps.append(nn(e.astype(BF16), all_values) / e.sum(axis=-1, keepdims=True))
    diff_out = maps[0] - diff_lambda[0] * maps[1]
    level = lax.rsqrt(jnp.mean(diff_out * diff_out, axis=-1, keepdims=True) + EPS)
    diff_mix = (diff_out * level * diff_gain).astype(BF16)

    mixed = jnp.concatenate([ret_mix, diff_mix], axis=1)
    partial = nn(mixed, full_weight).astype(BF16)
    shares = lax.all_to_all(partial, ("fs", "tp"), 0, 0, tiled=True)
    return shares.reshape(group, own_rows, width).astype(F32).sum(axis=0).astype(BF16)


def solution(mesh):
    count = mesh.shape["sp"]
    in_specs = (
        P(("sp", "fs", "tp"), None),
        P(),
        P(None, ("fs", "tp")),
        P(None, ("fs", "tp")),
        P(None, ("fs", "tp")),
        P(("fs", "tp"), "sp"),
        P(("fs", "tp"), None, None),
        P(("fs", "tp")),
        P(None, None, ("fs", "tp")),
        P(None, None, ("fs", "tp")),
        P(None, ("fs", "tp")),
        P(("fs", "tp")),
        P(("fs", "tp")),
        P(None, ("fs", "tp"), "sp"),
    )
    out_specs = P(("sp", "fs", "tp"), None)
    local = local_few if few(count) and mesh.shape["fs"] == 4 and mesh.shape["tp"] == 2 else local_many
    step = jax.shard_map(local, mesh=mesh, in_specs=in_specs, out_specs=out_specs, check_vma=False)
    if local is local_many:
        return step
    return step
```
